128 devices in a mesh: sp: 16 (over z, y), dp: 8 (over x, core).
Axes of the slice: x: 4, y: 4, z: 4, core: 2. Of those that a mesh axis runs over, the one named last changes fastest.
Arguments:
- residual: bfloat16 [8, 4096, 2048], P('dp', 'sp'), may hold values from -6 to 6
- queries: bfloat16 [8, 4096, 1024], P('dp', 'sp'), may hold values from -400 to 400
- key_vectors: bfloat16 [8, 4096, 1024], P('dp', 'sp'), may hold values from -6 to 6
- value_vectors: bfloat16 [8, 4096, 1024], P('dp', 'sp'), may hold values from -6 to 6
- gate_cache: float32 [8, 4096, 16], P('dp', 'sp'), may hold values from -514 to 0, as said below
- out_weight: bfloat16 [1024, 2048], P(None, 'dp'), may hold values from -0.1875 to 0.1875
- mix_gain: float32 [2048], replicated, may hold values from 0.1 to 1.9
- route_gain: float32 [2048], replicated, may hold values from 0.1 to 1.9
- out_gain: float32 [2048], replicated, may hold values from 0.1 to 1.9
- routes: int32 [8, 4096, 2], P('dp', 'sp'), may hold values from 0 to 15, all different within a row; in each aligned block of 256 rows (0 to 255, 256 to 511, ..., all dimensions but the last counted through in order) at most 64 rows name the same one
- group_share: float32 [8, 4096], P('dp', 'sp'), may hold values from 0.2 to 1
- expert_share: float32 [8, 4096, 2], P('dp', 'sp'), may hold values from 0.1 to 1
- gate_proj: bfloat16 [16, 2048, 1024], P('sp'), may hold values from -0.125 to 0.125
- up_proj: bfloat16 [16, 2048, 1024], P('sp'), may hold values from -0.125 to 0.125
- down_proj: bfloat16 [16, 1024, 2048], P('sp'), may hold values from -0.1875 to 0.1875
Outputs:
- layer_out: bfloat16 [8, 4096, 2048], P('dp', 'sp')
The draws below stay inside these ranges and needn't reach their ends.
Inputs may be any that keep to these rules, and one draw needn't show every extreme that they name: `gate_cache`: along the positions of a sequence the values never rise. `routes`: the 2 experts of a position differ. Within the rows of one device (aligned blocks of 256 positions) no expert is named more than 64 times, a bound that some block reaches.
All inputs are finite; a program needn't handle non-finite values.
Results may differ from the reference program's by a relative error of at most 0.0085.
Values may be sent and summed in bfloat16 or wider, within the bound.
No kernel may reach another device: no remote copies, remote signals or barrier semaphores. Data moves between devices by JAX's collectives and lax.ppermute only.
A program may use at most 128 MiB of HBM per device.

```python
import math
import jax
import jax.numpy as jnp
import numpy as np
from jax import lax

D = 2048
HEADS = 16
FF = 1024
TOP = 2
TOK_DEV = 256
ATTN = 1024
SEQUENCE_LENGTH = 4096
SEQUENCE_COUNT = 8
EXPERTS = 16
CAP = 64


def drawn_pair(base):
    key_draw = jnp.clip(jax.random.normal(jax.random.fold_in(base, 11), (SEQUENCE_COUNT, SEQUENCE_LENGTH, ATTN), jnp.float32), -6.0, 6.0)
    query_draw = jnp.clip(jax.random.normal(jax.random.fold_in(base, 12), (SEQUENCE_COUNT, SEQUENCE_LENGTH, ATTN), jnp.float32), -6.0, 6.0)
    return (query_draw, key_draw)


def draw_queries(key, part):
    return drawn_pair(key)[0].astype(jnp.bfloat16)


def draw_key_vectors(key, part):
    return drawn_pair(key)[1].astype(jnp.bfloat16)


def draw_gate_cache(key, part):
    picks = jax.random.permutation(jax.random.fold_in(key, 21), HEADS)
    lagging_heads = (picks < HEADS // 2).astype(jnp.float32)
    fast_rate = jnp.exp(jax.random.uniform(jax.random.fold_in(key, 22), (HEADS,), jnp.float32, math.log(0.01), math.log(0.033)))
    decay_rate = lagging_heads * (0.6 / SEQUENCE_LENGTH) + (1.0 - lagging_heads) * fast_rate
    coarse_estimate = jax.random.uniform(jax.random.fold_in(key, 23), (SEQUENCE_COUNT, SEQUENCE_LENGTH, HEADS), jnp.float32, 0.3, 1.7)
    block_count = SEQUENCE_LENGTH // TOK_DEV
    multiplier = jnp.exp(jax.random.uniform(jax.random.fold_in(key, 24), (SEQUENCE_COUNT, block_count, 1, 1), jnp.float32, math.log(0.5), math.log(2.0)))
    multiplier = jnp.broadcast_to(multiplier, (SEQUENCE_COUNT, block_count, TOK_DEV, 1)).reshape(SEQUENCE_COUNT, SEQUENCE_LENGTH, 1)
    spike_position = jax.random.randint(jax.random.fold_in(key, 25), (SEQUENCE_COUNT, 1, 2), 1, SEQUENCE_LENGTH)
    spike_length = jax.random.uniform(jax.random.fold_in(key, 26), (SEQUENCE_COUNT, 1, 2), jnp.float32, 0.22, 0.69)
    token_position = jnp.arange(SEQUENCE_LENGTH)[None, :, None]
    spike_value = jnp.sum(jnp.where(token_position == spike_position, spike_length, 0.0), axis=2, keepdims=True)
    gate_logarithm = -decay_rate[None, None, :] * coarse_estimate * multiplier - spike_value * lagging_heads[None, None, :]
    return jnp.cumsum(gate_logarithm, axis=1).astype(jnp.float32)


def levels(stream_key, dims, pieces, smallest, high):
    level, own = 1.0, jax.random.fold_in(stream_key, 6)
    for axis_at, shards_of in pieces:
        steps = jnp.exp(jax.random.uniform(jax.random.fold_in(own, axis_at), (shards_of,), jnp.float32, smallest / len(pieces), high / len(pieces)))
        level = level * jnp.repeat(steps, dims[axis_at] // shards_of).reshape([-1 if axis == axis_at else 1 for axis in range(len(dims))])
    return level


def assign_block(stream_key, own, number, rows, amount, top, bound, slope):
    order = jax.random.permutation(stream_key, amount)
    packed, common = portions_of(amount, rows * top, bound, slope, True), portions_of(amount, rows * top, bound, slope, False)
    places = jnp.arange(amount)

    def named(sizes, offset_by):
        used = int((sizes > 0).sum())
        fixed = max(1, used // 4)
        passed = fixed + (places - fixed + offset_by * (used - fixed)) % max(1, amount - fixed)
        return jnp.zeros((amount,), jnp.int32).at[order[jnp.where(places < fixed, places, passed)]].set(jnp.asarray(sizes, jnp.int32))

    sizes = jnp.where(number % 4 == 0, named(packed, number // 4), named(common, number - number // 4 - 1))
    mixed = jax.random.permutation(jax.random.fold_in(own, 3), amount)
    donor, receiver = mixed[0:amount // 2 * 2:2], mixed[1:amount // 2 * 2:2]
    margin = jnp.minimum(sizes[donor] - 1, bound - sizes[receiver]) // 2
    margin = jnp.where((donor == order[0]) | (receiver == order[0]) | (sizes[receiver] == 0), 0, jnp.maximum(margin, 0))
    passed = jax.random.randint(jax.random.fold_in(own, 4), (amount // 2,), 0, 1 << 20) % (margin + 1)
    sizes = sizes.at[donor].add(-passed).at[receiver].add(passed)
    labels = jnp.searchsorted(jnp.cumsum(sizes), jnp.arange(rows * top), side="right").astype(jnp.int32)
    listing = labels.reshape(top, rows).T
    listing = listing[jax.random.permutation(jax.random.fold_in(own, 1), rows)]
    offset_by = jax.random.randint(jax.random.fold_in(own, 2), (rows, 1), 0, top)
    return jnp.take_along_axis(listing, (jnp.arange(top)[None, :] + offset_by) % top, axis=1)


def portions_of(amount, total, most, slope, full):
    loads = [(1 << 20) // math.isqrt(standing ** slope) + 1 for standing in range(1, amount + 1)]
    largest = most if full else min(most, max(-(-total // amount), total * loads[0] // sum(loads)))
    least = 1 if total - largest >= amount - 1 else 0
    given, rest = [largest] + [least] * (amount - 1), total - largest - least * (amount - 1)
    while rest > 0:
        movable = [i for i in range(1, amount) if given[i] < largest] or [i for i in range(1, amount) if given[i] < most]
        pool, remaining = sum([loads[i] for i in movable]), rest
        for i in movable:
            more = min(most - given[i], max(1, remaining * loads[i] // pool), rest)
            given[i] = given[i] + more
            rest = rest - more
    return np.array(given)


def bell_draw(stream_key, dims, spread, bound, cuts=(), held_as=jnp.bfloat16):
    loudness = levels(stream_key, dims, cuts, -0.22, 0.18) if cuts else 1.0
    values = jax.random.normal(stream_key, dims, jnp.float32) * spread * loudness
    return jnp.minimum(jnp.maximum(values, -bound), bound).astype(held_as)


def setup_inputs(seed: int = 0) -> dict:
    splits = jax.random.split(jax.random.key(seed), 16)
    residual = bell_draw(splits[0], (SEQUENCE_COUNT, SEQUENCE_LENGTH, D), 1.0, 6.0, ((0, 8), (1, 16)))
    queries = draw_queries(jax.random.fold_in(splits[15], 71), 0)
    key_vectors = draw_key_vectors(jax.random.fold_in(splits[15], 71), 0)
    value_vectors = bell_draw(splits[3], (SEQUENCE_COUNT, SEQUENCE_LENGTH, ATTN), 1.0, 6.0, ((0, 8), (1, 16)))
    gate_cache = draw_gate_cache(jax.random.fold_in(splits[15], 71), 0)
    out_weight = bell_draw(splits[5], (ATTN, D), ATTN ** -0.5, 0.1875, ((1, 8),))
    mix_gain = jnp.clip(1.0 + 0.18 * jax.random.normal(splits[6], (D,), jnp.float32), 0.1, 1.9)
    route_gain = jnp.clip(1.0 + 0.18 * jax.random.normal(splits[7], (D,), jnp.float32), 0.1, 1.9)
    out_gain = jnp.clip(1.0 + 0.18 * jax.random.normal(splits[8], (D,), jnp.float32), 0.1, 1.9)
    routes_keys = jax.random.split(jax.random.fold_in(splits[9], 1), SEQUENCE_COUNT * SEQUENCE_LENGTH // TOK_DEV)
    routes_turns = jax.random.permutation(jax.random.fold_in(splits[9], 3), SEQUENCE_COUNT * SEQUENCE_LENGTH // TOK_DEV)
    routes = jax.vmap(lambda own, number: assign_block(jax.random.fold_in(splits[9], 2), own, number, TOK_DEV, EXPERTS, TOP, CAP, 2))(routes_keys, routes_turns).reshape((SEQUENCE_COUNT, SEQUENCE_LENGTH, TOP))
    group_share = jnp.clip(jnp.exp(math.log(1.0) - 1.609438 * jax.random.uniform(splits[10], (SEQUENCE_COUNT, SEQUENCE_LENGTH), jnp.float32) ** levels(splits[10], (SEQUENCE_COUNT, SEQUENCE_LENGTH), ((0, 8), (1, 16)), -0.2, 0.2)), 0.2, 1.0)
    expert_share = jnp.clip(jnp.exp(math.log(1.0) - 2.3025851 * jax.random.uniform(splits[11], (SEQUENCE_COUNT, SEQUENCE_LENGTH, TOP), jnp.float32) ** levels(splits[11], (SEQUENCE_COUNT, SEQUENCE_LENGTH, TOP), ((0, 8), (1, 16)), -0.2, 0.2)), 0.1, 1.0)
    gate_proj = bell_draw(splits[12], (EXPERTS, D, FF), D ** -0.5, 0.125, ((0, 16),))
    up_proj = bell_draw(splits[13], (EXPERTS, D, FF), D ** -0.5, 0.125, ((0, 16),))
    down_proj = bell_draw(splits[14], (EXPERTS, FF, D), FF ** -0.5, 0.1875, ((0, 16),))
    return {"residual": residual, "queries": queries, "key_vectors": key_vectors, "value_vectors": value_vectors, "gate_cache": gate_cache, "out_weight": out_weight, "mix_gain": mix_gain, "route_gain": route_gain, "out_gain": out_gain, "routes": routes, "group_share": group_share, "expert_share": expert_share, "gate_proj": gate_proj, "up_proj": up_proj, "down_proj": down_proj}


def normalize(values):
    return values * lax.rsqrt(lax.optimization_barrier(jnp.mean(values * values, axis=-1, keepdims=True)) + 1e-06)

def attend(queries, key_vectors, value_vectors, cum_gates):
    length = queries.shape[0]
    head_count = cum_gates.shape[1]
    head_width = queries.shape[1] // head_count
    score_scale = head_width ** (-0.5)
    q_heads = queries.reshape(length, head_count, head_width).astype(jnp.float32)
    k_heads = key_vectors.reshape(length, head_count, head_width).astype(jnp.float32)
    v_heads = value_vectors.reshape(length, head_count, head_width).astype(jnp.float32)
    block_rows = min(512, length)
    outputs = []
    for offset in range(0, length, block_rows):
        stop = offset + block_rows
        scores = jnp.einsum('qhd,khd->hqk', q_heads[offset:stop], k_heads[:stop]) * score_scale
        bias = cum_gates[offset:stop].T[:, :, None] - cum_gates[:stop].T[:, None, :]
        row_pos = offset + jnp.arange(block_rows, dtype=jnp.int32)[:, None]
        col_pos = jnp.arange(stop, dtype=jnp.int32)[None, :]
        scores = jnp.where(col_pos <= row_pos, scores + bias, -1e+30)
        row_max = lax.optimization_barrier(jnp.max(scores, axis=-1, keepdims=True))
        expo_terms = jnp.exp(scores - row_max)
        probs = (expo_terms / lax.optimization_barrier(jnp.sum(expo_terms, axis=-1, keepdims=True))).astype(jnp.bfloat16)
        mixing = jnp.einsum('hqk,khd->qhd', probs.astype(jnp.float32), v_heads[:stop])
        outputs.append(mixing.astype(jnp.bfloat16).reshape(block_rows, head_count * head_width))
    return jnp.concatenate(outputs, axis=0)

def reference(residual, queries, key_vectors, value_vectors, gate_cache, out_weight, mix_gain, route_gain, out_gain, routes, group_share, expert_share, gate_proj, up_proj, down_proj):
    seq_count, length, model_width = residual.shape
    tokens = seq_count * length

    def one_sequence(operands):
        return attend(operands[0], operands[1], operands[2], operands[3])
    attended = lax.map(one_sequence, (queries, key_vectors, value_vectors, gate_cache))
    mixed = jnp.dot(attended.reshape(tokens, -1), out_weight, preferred_element_type=jnp.float32)
    hidden = (residual.reshape(tokens, model_width).astype(jnp.float32) + normalize(mixed) * mix_gain).astype(jnp.bfloat16)
    routed = (normalize(hidden.astype(jnp.float32)) * route_gain).astype(jnp.bfloat16)
    experts = gate_proj.shape[0]
    blocks = tokens // TOK_DEV
    count = TOK_DEV * TOP
    assigned = routes.reshape(blocks, count)
    expert_ids = jnp.arange(experts, dtype=jnp.int32)
    one_hot = (assigned[:, :, None] == expert_ids[None, None, :]).astype(jnp.int32)
    ranking = lax.optimization_barrier(jnp.sum((jnp.cumsum(one_hot, axis=1) - one_hot) * one_hot, axis=2))
    slot_index = assigned * CAP + ranking
    owners = jnp.broadcast_to(jnp.arange(count, dtype=jnp.int32)[None, :] // TOP, (blocks, count))
    block_ids = jnp.arange(blocks, dtype=jnp.int32)[:, None]
    shares = expert_share.reshape(tokens, TOP)
    weights = group_share.reshape(tokens, 1) * shares / lax.optimization_barrier(jnp.sum(shares, axis=1, keepdims=True))
    slot_token = jnp.full((blocks, experts * CAP), TOK_DEV, jnp.int32).at[block_ids, slot_index].set(owners)
    slot_weight = jnp.zeros((blocks, experts * CAP), jnp.float32).at[block_ids, slot_index].set(weights.reshape(blocks, count))
    padded = jnp.concatenate([routed.reshape(blocks, TOK_DEV, model_width), jnp.zeros((blocks, 1, model_width), jnp.bfloat16)], axis=1)

    def one_expert(totals, operands):
        w_gate, w_up, w_down, expert_index = operands
        tok_index = lax.dynamic_slice_in_dim(slot_token, expert_index * CAP, CAP, 1)
        w_slots = lax.dynamic_slice_in_dim(slot_weight, expert_index * CAP, CAP, 1)
        rows_in = padded[block_ids, tok_index].reshape(blocks * CAP, model_width)
        gate = jnp.dot(rows_in, w_gate, preferred_element_type=jnp.float32)
        upper = jnp.dot(rows_in, w_up, preferred_element_type=jnp.float32)
        act = (jax.nn.silu(gate) * upper).astype(jnp.bfloat16)
        result = jnp.dot(act, w_down, preferred_element_type=jnp.float32).astype(jnp.bfloat16)
        result = result.reshape(blocks, CAP, model_width).astype(jnp.float32)
        totals = totals.at[block_ids, tok_index].add(w_slots[:, :, None] * result)
        return (totals, None)
    start_totals = jnp.zeros((blocks, TOK_DEV + 1, model_width), jnp.float32)
    totals, unused = lax.scan(one_expert, start_totals, (gate_proj, up_proj, down_proj, jnp.arange(experts, dtype=jnp.int32)))
    combined = totals[:, :TOK_DEV].reshape(tokens, model_width)
    layer_out = (hidden.astype(jnp.float32) + combined * out_gain).astype(jnp.bfloat16)
    return layer_out.reshape(seq_count, length, model_width)
```

```python
import jax
import jax.numpy as jnp
from jax import lax
from jax.experimental import pallas as pl
from jax.experimental.pallas import tpu as pltpu
from jax.sharding import PartitionSpec as P

F32 = jnp.float32
BF16 = jnp.bfloat16
HD = 64
SLOTS = 64
NEG = -1e30


def vmem(mib):
    return pltpu.CompilerParams(vmem_limit_bytes=mib * 1024 * 1024)


def vspec():
    return pl.BlockSpec(memory_space=pltpu.VMEM)


def pack_kernel(q_ref, k_ref, v_ref, g_ref, o_ref):
    rows = q_ref.shape[0]
    half = rows // 2
    heads = g_ref.shape[1]
    gates = jnp.concatenate([g_ref[...], jnp.zeros((rows, 128 - heads), F32)], axis=1).T
    hi = gates.astype(BF16).astype(F32)
    mid = (gates - hi).astype(BF16).astype(F32)
    low = gates - hi - mid
    for pair in range(heads // 2):
        cols = slice(128 * pair, 128 * pair + 128)
        q, k, v = q_ref[:, cols], k_ref[:, cols], v_ref[:, cols]
        for side in range(2):
            h = 2 * pair + side
            at = slice(64 * side, 64 * side + 64)
            o_ref[h, 0:rows, :] = jnp.concatenate([q[:, at], k[:, at]], axis=1)
            o_ref[h, rows:rows + half, :] = jnp.concatenate([v[:half, at], v[half:, at]], axis=1)
            terms = [t[h:h + 1, 128 * j:128 * j + 128] for t in (hi, mid, low) for j in range(2)]
            terms.append(jnp.zeros((10, 128), F32))
            o_ref[h, rows + half:rows + half + 16, :] = jnp.concatenate(terms, axis=0).astype(BF16)


def pack(q, k, v, g):
    rows, heads = q.shape[0], g.shape[1]
    return pl.pallas_call(
        pack_kernel,
        out_shape=jax.ShapeDtypeStruct((heads, rows + rows // 2 + 16, 128), BF16),
        in_specs=[vspec()] * 4,
        out_specs=vspec(),
        compiler_params=vmem(40),
        name="pack",
    )(q, k, v, g)


def attend_kernel(x_ref, o_ref, q_scr, k_scr, v_scr, g_scr, s_scr):
    blocks = x_ref.shape[0]
    rows = (x_ref.shape[1] - 16) * 2 // 3
    half = rows // 2
    lane = lax.broadcasted_iota(jnp.int32, (128, 64), 1)
    lane2 = lax.broadcasted_iota(jnp.int32, (rows, 64), 1)
    minus = jnp.where(lane2 < 3, -1.0, 0.0).astype(BF16)
    ones = jnp.where(lane2 < 1, 1.0, 0.0).astype(BF16)
    g_scr[...] = jnp.zeros_like(g_scr)
    for b in range(blocks):
        t = x_ref[b, rows + half:rows + half + 16, :].astype(F32)
        g_scr[2 * b:2 * b + 2, :] = t[0:2] + t[2:4] + t[4:6]
    gates = g_scr[...].T
    for b in range(blocks):
        base = b * rows
        qk = x_ref[b, 0:rows, :]
        q = (qk[:, 0:64].astype(F32) * (HD ** -0.5)).astype(BF16)
        q_scr[base:base + rows, :] = jnp.concatenate([q, minus], axis=1)
        for j in range(2):
            c = gates[:, 2 * b + j:2 * b + j + 1]
            hi = c.astype(BF16).astype(F32)
            mid = (c - hi).astype(BF16).astype(F32)
            low = c - hi - mid
            ext = jnp.where(lane == 0, hi, jnp.where(lane == 1, mid, jnp.where(lane == 2, low, 0.0)))
            k_scr[base + 128 * j:base + 128 * j + 128, :] = jnp.concatenate(
                [qk[128 * j:128 * j + 128, 64:128], ext.astype(BF16)], axis=1)
        vv = x_ref[b, rows:rows + half, :]
        v_scr[base:base + half, :] = jnp.concatenate([vv[:, 0:64], ones[:half]], axis=1)
        v_scr[base + half:base + rows, :] = jnp.concatenate([vv[:, 64:128], ones[:half]], axis=1)

    tile = 2 * rows
    nt = (((1,), (1,)), ((), ()))

    def top_of(s):
        m = s[:, 0:128]
        for j in range(1, tile // 128):
            m = jnp.maximum(m, s[:, 128 * j:128 * j + 128])
        return m

    def q_tile(qi, _):
        q = q_scr[pl.ds(qi * tile, tile), :]

        def scores(kj, m):
            s = lax.dot_general(q, k_scr[pl.ds(kj * tile, tile), :], nt, preferred_element_type=F32)
            s_scr[kj] = s
            return jnp.maximum(m, top_of(s))

        m = lax.fori_loop(0, qi, scores, jnp.full((tile, 128), NEG, F32))
        s = lax.dot_general(q, k_scr[pl.ds(qi * tile, tile), :], nt, preferred_element_type=F32)
        r = lax.broadcasted_iota(jnp.int32, (tile, tile), 0)
        c = lax.broadcasted_iota(jnp.int32, (tile, tile), 1)
        s = jnp.where(c <= r, s, NEG)
        m = jnp.max(jnp.maximum(m, top_of(s)), axis=1, keepdims=True)
        p = jnp.exp(s - m).astype(BF16)
        acc = jnp.dot(p, v_scr[pl.ds(qi * tile, tile), :], preferred_element_type=F32)

        def mixing(kj, acc):
            p = jnp.exp(s_scr[kj] - m).astype(BF16)
            return acc + jnp.dot(p, v_scr[pl.ds(kj * tile, tile), :], preferred_element_type=F32)

        acc = lax.fori_loop(0, qi, mixing, acc)
        out = acc[:, 0:64] / acc[:, 64:65]
        for j in range(2):
            top = out[j * rows:j * rows + half]
            bottom = out[j * rows + half:(j + 1) * rows]
            o_ref[2 * qi + j] = jnp.concatenate([top, bottom], axis=1).astype(BF16)
        return 0

    lax.fori_loop(0, blocks // 2, q_tile, 0)


def attend(x):
    blocks = x.shape[0]
    rows = (x.shape[1] - 16) * 2 // 3
    length = blocks * rows
    return pl.pallas_call(
        attend_kernel,
        out_shape=jax.ShapeDtypeStruct((blocks, rows // 2, 128), BF16),
        in_specs=[vspec()],
        out_specs=vspec(),
        scratch_shapes=[
            pltpu.VMEM((length, 128), BF16),
            pltpu.VMEM((length, 128), BF16),
            pltpu.VMEM((length, 128), BF16),
            pltpu.VMEM((128, 128), F32),
            pltpu.VMEM((blocks // 2, 2 * rows, 2 * rows), F32),
        ],
        compiler_params=vmem(48),
        name="attend",
    )(x)


def route_kernel(r_ref, gs_ref, es_ref, pa_ref, pb_ref, ca_ref, cb_ref):
    rows = r_ref.shape[0]
    experts = pa_ref.shape[0] // (SLOTS // 2)
    half = SLOTS // 2
    e0, e1 = r_ref[:, 0:1], r_ref[:, 1:2]
    lane = lax.broadcasted_iota(jnp.int32, (rows, 128), 1)
    named = jnp.where((lane == e0) | (lane == e1), 1.0, 0.0)
    ri = lax.broadcasted_iota(jnp.int32, (rows, rows), 0)
    ci = lax.broadcasted_iota(jnp.int32, (rows, rows), 1)
    before = jnp.where(ci < ri, 1.0, 0.0).astype(BF16)
    rank = jnp.dot(before, named.astype(BF16), preferred_element_type=F32)
    place = jnp.where(named > 0, rank, -1.0)
    by_expert = place.T
    slot_row = lax.broadcasted_iota(jnp.int32, (half, rows), 0).astype(F32)
    for e in range(experts):
        mine = by_expert[e:e + 1, :]
        pa_ref[e * half:(e + 1) * half, :] = jnp.where(mine == slot_row, 1.0, 0.0).astype(BF16)
        pb_ref[e * half:(e + 1) * half, :] = jnp.where(mine == slot_row + half, 1.0, 0.0).astype(BF16)
    share = jnp.sum(jnp.where(ri == ci, gs_ref[...], 0.0), axis=1, keepdims=True)
    s0, s1 = es_ref[:, 0:1], es_ref[:, 1:2]
    total = s0 + s1
    w0, w1 = share * s0 / total, share * s1 / total
    k0 = jnp.sum(jnp.where(lane == e0, rank, 0.0), axis=1, keepdims=True).astype(jnp.int32)
    k1 = jnp.sum(jnp.where(lane == e1, rank, 0.0), axis=1, keepdims=True).astype(jnp.int32)
    at = lax.broadcasted_iota(jnp.int32, (rows, experts * half), 1)
    for ref, low in ((ca_ref, 0), (cb_ref, half)):
        a0 = jnp.where((k0 >= low) & (k0 < low + half), e0 * half + k0 - low, -1)
        a1 = jnp.where((k1 >= low) & (k1 < low + half), e1 * half + k1 - low, -1)
        w = jnp.where(at == a0, w0, jnp.where(at == a1, w1, 0.0))
        hi = w.astype(BF16)
        ref[0:rows, :] = hi
        ref[rows:2 * rows, :] = (w - hi.astype(F32)).astype(BF16)


def route_tables(routes, group_share, expert_share, experts):
    rows = routes.shape[0]
    n = experts * SLOTS // 2
    p_shape = jax.ShapeDtypeStruct((n, rows), BF16)
    c_shape = jax.ShapeDtypeStruct((2 * rows, n), BF16)
    return pl.pallas_call(
        route_kernel,
        out_shape=(p_shape, p_shape, c_shape, c_shape),
        in_specs=[vspec()] * 3,
        out_specs=(vspec(),) * 4,
        compiler_params=vmem(32),
        name="route_tables",
    )(routes, group_share, expert_share)


def project_kernel(a_ref, w_ref, res_ref, mg_ref, rg_ref, p_ref, hid_ref, routed_ref, out_ref):
    heads, half = a_ref.shape[0], a_ref.shape[1]
    left = lax.broadcasted_iota(jnp.int32, (half, 128), 1) < 64
    tops, bottoms = [], []
    for pair in range(heads // 2):
        a = a_ref[2 * pair]
        b = a_ref[2 * pair + 1]
        tops.append(jnp.concatenate([a[:, 0:64], b[:, 0:64]], axis=1))
        bottoms.append(jnp.concatenate([a[:, 64:128], b[:, 64:128]], axis=1))
    att = jnp.concatenate([jnp.concatenate(tops, axis=1), jnp.concatenate(bottoms, axis=1)], axis=0)
    mixed = jnp.dot(att, w_ref[...], preferred_element_type=F32)
    scale = lax.rsqrt(jnp.mean(mixed * mixed, axis=1, keepdims=True) + 1e-6)
    hidden = (res_ref[...].astype(F32) + mixed * scale * mg_ref[...]).astype(BF16)
    hid_ref[...] = hidden
    h = hidden.astype(F32)
    routed = (h * lax.rsqrt(jnp.mean(h * h, axis=1, keepdims=True) + 1e-6) * rg_ref[...]).astype(BF16)
    routed_ref[...] = routed
    out_ref[...] = jnp.dot(p_ref[...], routed, preferred_element_type=F32).astype(BF16)


def project(att, weight, residual, mix_gain, route_gain, table):
    rows, width = residual.shape
    flat = jax.ShapeDtypeStruct((rows, width), BF16)
    return pl.pallas_call(
        project_kernel,
        out_shape=(flat, flat, jax.ShapeDtypeStruct((table.shape[0], width), BF16)),
        in_specs=[vspec()] * 6,
        out_specs=(vspec(),) * 3,
        compiler_params=vmem(48),
        name="project",
    )(att, weight, residual, mix_gain, route_gain, table)


def select_kernel(p_ref, x_ref, o_ref):
    o_ref[...] = jnp.dot(p_ref[...], x_ref[...], preferred_element_type=F32).astype(BF16)


def select_rows(table, x):
    return pl.pallas_call(
        select_kernel,
        out_shape=jax.ShapeDtypeStruct((table.shape[0], x.shape[1]), BF16),
        in_specs=[vspec()] * 2,
        out_specs=vspec(),
        compiler_params=vmem(32),
        name="select_rows",
    )(table, x)


def expert_kernel(x_ref, g_ref, u_ref, d_ref, o_ref, act_scr, acc_scr):
    f = pl.program_id(0)
    x = x_ref[...]
    gate = jnp.dot(x, g_ref[...], preferred_element_type=F32)
    upper = jnp.dot(x, u_ref[...], preferred_element_type=F32)
    act = (gate / (1.0 + jnp.exp(-gate)) * upper).astype(BF16)
    part = jnp.dot(act, d_ref[...], preferred_element_type=F32)

    @pl.when(f == 0)
    def _():
        acc_scr[...] = part

    @pl.when((f > 0) & (f < pl.num_programs(0) - 1))
    def _():
        acc_scr[...] += part

    @pl.when(f == pl.num_programs(0) - 1)
    def _():
        o_ref[...] = (acc_scr[...] + part).astype(BF16)


def expert(x, gate, up, down, tile=512):
    rows, width = x.shape
    ff = gate.shape[1]
    return pl.pallas_call(
        expert_kernel,
        grid=(ff // tile,),
        out_shape=jax.ShapeDtypeStruct((rows, width), BF16),
        in_specs=[
            pl.BlockSpec((rows, width), lambda f: (0, 0)),
            pl.BlockSpec((width, tile), lambda f: (0, f)),
            pl.BlockSpec((width, tile), lambda f: (0, f)),
            pl.BlockSpec((tile, width), lambda f: (f, 0)),
        ],
        out_specs=pl.BlockSpec((rows, width), lambda f: (0, 0)),
        scratch_shapes=[pltpu.VMEM((8, 128), BF16), pltpu.VMEM((rows, width), F32)],
        compiler_params=vmem(56),
        cost_estimate=pl.CostEstimate(flops=6 * rows * width * ff, transcendentals=rows * ff, bytes_accessed=16000000),
        name="expert",
    )(x, gate, up, down)


def gather_kernel(c_ref, x_ref, o_ref):
    rows = o_ref.shape[0]
    both = jnp.dot(c_ref[...], x_ref[...], preferred_element_type=F32)
    o_ref[...] = both[:rows] + both[rows:]


def gather_sum(table, x):
    return pl.pallas_call(
        gather_kernel,
        out_shape=jax.ShapeDtypeStruct((table.shape[0] // 2, x.shape[1]), F32),
        in_specs=[vspec()] * 2,
        out_specs=vspec(),
        compiler_params=vmem(32),
        name="gather_sum",
    )(table, x)


def finish_kernel(c_ref, x_ref, first_ref, hid_ref, og_ref, o_ref):
    rows = o_ref.shape[0]
    both = jnp.dot(c_ref[...], x_ref[...], preferred_element_type=F32)
    combined = first_ref[...] + both[:rows] + both[rows:]
    o_ref[...] = (hid_ref[...].astype(F32) + combined * og_ref[...]).astype(BF16)


def finish(table, x, first, hidden, out_gain):
    return pl.pallas_call(
        finish_kernel,
        out_shape=jax.ShapeDtypeStruct(hidden.shape, BF16),
        in_specs=[vspec()] * 5,
        out_specs=vspec(),
        compiler_params=vmem(40),
        name="finish",
    )(table, x, first, hidden, out_gain)


def swap(x):
    return lax.all_to_all(x, "sp", split_axis=0, concat_axis=0, tiled=True)


def body(
    residual,
    queries,
    key_vectors,
    value_vectors,
    gate_cache,
    out_weight,
    mix_gain,
    route_gain,
    out_gain,
    routes,
    group_share,
    expert_share,
    gate_proj,
    up_proj,
    down_proj,
):
    experts = lax.axis_size("sp")
    width = residual.shape[2]
    weight = lax.all_gather(out_weight, "dp", axis=1, tiled=True)
    arrived = swap(pack(queries[0], key_vectors[0], value_vectors[0], gate_cache[0]))
    pa, pb, ca, cb = route_tables(routes[0], group_share, expert_share[0], experts)
    att = swap(attend(arrived))
    hidden, routed, rows_a = project(
        att, weight, residual[0], mix_gain[None], route_gain[None], pa)

    def exchange(x):
        return swap(x.reshape(experts, SLOTS // 2, width)).reshape(x.shape)

    in_a = exchange(rows_a)
    in_b = exchange(select_rows(pb, routed))
    out_a = exchange(expert(in_a, gate_proj[0], up_proj[0], down_proj[0]))
    out_b = exchange(expert(in_b, gate_proj[0], up_proj[0], down_proj[0]))
    first = gather_sum(ca, out_a)
    return finish(cb, out_b, first, hidden, out_gain[None])[None]


def solution(mesh):
    placed = (
        P("dp", "sp", None),
        P("dp", "sp", None),
        P("dp", "sp", None),
        P("dp", "sp", None),
        P("dp", "sp", None),
        P(None, "dp"),
        P(),
        P(),
        P(),
        P("dp", "sp", None),
        P("dp", "sp"),
        P("dp", "sp", None),
        P("sp", None, None),
        P("sp", None, None),
        P("sp", None, None),
    )
    return jax.shard_map(
        body, mesh=mesh, in_specs=placed, out_specs=P("dp", "sp", None), check_vma=False
    )
```

```python
import jax
import jax.numpy as jnp
from jax import lax
from jax.experimental import pallas as pl
from jax.experimental.pallas import tpu as pltpu
from jax.sharding import PartitionSpec as P

F32 = jnp.float32
BF16 = jnp.bfloat16
HD = 64
SLOTS = 64
NEG = -1e30


def vmem(mib):
    return pltpu.CompilerParams(vmem_limit_bytes=mib * 1024 * 1024)


def vspec():
    return pl.BlockSpec(memory_space=pltpu.VMEM)


def pack_kernel(q_ref, k_ref, v_ref, g_ref, o_ref):
    rows = q_ref.shape[0]
    half = rows // 2
    heads = g_ref.shape[1]
    gates = jnp.concatenate([g_ref[...], jnp.zeros((rows, 128 - heads), F32)], axis=1).T
    hi = gates.astype(BF16).astype(F32)
    mid = (gates - hi).astype(BF16).astype(F32)
    low = gates - hi - mid
    for pair in range(heads // 2):
        cols = slice(128 * pair, 128 * pair + 128)
        q, k, v = q_ref[:, cols], k_ref[:, cols], v_ref[:, cols]
        for side in range(2):
            h = 2 * pair + side
            at = slice(64 * side, 64 * side + 64)
            o_ref[h, 0:rows, :] = jnp.concatenate([q[:, at], k[:, at]], axis=1)
            o_ref[h, rows:rows + half, :] = jnp.concatenate([v[:half, at], v[half:, at]], axis=1)
            terms = [t[h:h + 1, 128 * j:128 * j + 128] for t in (hi, mid, low) for j in range(2)]
            terms.append(jnp.zeros((10, 128), F32))
            o_ref[h, rows + half:rows + half + 16, :] = jnp.concatenate(terms, axis=0).astype(BF16)


def pack(q, k, v, g):
    rows, heads = q.shape[0], g.shape[1]
    return pl.pallas_call(
        pack_kernel,
        out_shape=jax.ShapeDtypeStruct((heads, rows + rows // 2 + 16, 128), BF16),
        in_specs=[vspec()] * 4,
        out_specs=vspec(),
        compiler_params=vmem(40),
        name="pack",
    )(q, k, v, g)


TILE = 512


def attend_kernel(x_ref, o_ref, q_scr, k_scr, v_scr, buf_a, buf_b):
    blocks = x_ref.shape[0]
    rows = (x_ref.shape[1] - 16) * 2 // 3
    half = rows // 2
    lane = lax.broadcasted_iota(jnp.int32, (rows, 64), 1)
    minus = jnp.where(lane < 3, -1.0, 0.0).astype(BF16)
    ones = jnp.where(lane < 1, 1.0, 0.0).astype(BF16)
    pr = lax.broadcasted_iota(jnp.int32, (16, 128), 0)
    pc = lax.broadcasted_iota(jnp.int32, (16, 128), 1)
    picks = [
        jnp.where((pr == 2 * (pc - 64) + j) & (pc >= 64) & (pc < 67), 1.0, 0.0).astype(BF16)
        for j in range(2)
    ]
    nt = (((1,), (1,)), ((), ()))
    tn = (((0,), (0,)), ((), ()))

    def prepare(b):
        base = b * rows
        qk = x_ref[b, 0:rows, :]
        q = (qk[:, 0:64].astype(F32) * (HD ** -0.5)).astype(BF16)
        q_scr[base:base + rows, :] = jnp.concatenate([q, minus], axis=1)
        terms = x_ref[b, rows + half:rows + half + 16, :]
        for j in range(2):
            ext = lax.dot_general(terms, picks[j], tn, preferred_element_type=F32).astype(BF16)
            at = slice(half * j, half * j + half)
            k_scr[base + half * j:base + half * j + half, :] = jnp.concatenate(
                [qk[at, 64:128], ext[:, 64:128]], axis=1)
        v = x_ref[b, rows:rows + half, :]
        v_scr[base:base + half, :] = jnp.concatenate([v[:, 0:64], ones[:half]], axis=1)
        v_scr[base + half:base + rows, :] = jnp.concatenate([v[:, 64:128], ones[:half]], axis=1)

    def score(q0, qn, k0, kn):
        return lax.dot_general(
            q_scr[q0:q0 + qn, :], k_scr[k0:k0 + kn, :], nt, preferred_element_type=F32)

    def top_of(s, m=None):
        for j in range(s.shape[1] // 128):
            t = s[:, 128 * j:128 * j + 128]
            m = t if m is None else jnp.maximum(m, t)
        return m

    def masked(s, off):
        r = lax.broadcasted_iota(jnp.int32, s.shape, 0) + off
        c = lax.broadcasted_iota(jnp.int32, s.shape, 1)
        return jnp.where(c <= r, s, NEG)

    hq = TILE // 2

    def scores_of(qi, buf):
        q0, m = qi * TILE, None
        for k0 in range(0, q0, TILE):
            s = score(q0, TILE, k0, TILE)
            buf[:, k0:k0 + TILE] = s
            m = top_of(s, m)
            yield m
        s1 = masked(score(q0, hq, q0, hq), 0)
        s2 = masked(score(q0 + hq, hq, q0, TILE), hq)
        buf[0:hq, q0:q0 + hq] = s1
        buf[hq:TILE, q0:q0 + TILE] = s2
        d = jnp.concatenate([top_of(s1), top_of(s2)], axis=0)
        yield d if m is None else jnp.maximum(m, d)

    def mix_of(qi, buf, m):
        q0 = qi * TILE
        acc = jnp.zeros((TILE, 128), F32)
        for k0 in range(0, q0, TILE):
            p = jnp.exp(buf[:, k0:k0 + TILE] - m).astype(BF16)
            acc = acc + jnp.dot(p, v_scr[k0:k0 + TILE, :], preferred_element_type=F32)
            yield acc
        p1 = jnp.exp(buf[0:hq, q0:q0 + hq] - m[0:hq]).astype(BF16)
        p2 = jnp.exp(buf[hq:TILE, q0:q0 + TILE] - m[hq:]).astype(BF16)
        a1 = jnp.dot(p1, v_scr[q0:q0 + hq, :], preferred_element_type=F32)
        a2 = jnp.dot(p2, v_scr[q0:q0 + TILE, :], preferred_element_type=F32)
        yield acc + jnp.concatenate([a1, a2], axis=0)

    per = TILE // rows

    def store(qi, acc):
        out = acc[:, 0:64] * (1.0 / acc[:, 64:65])
        for j in range(per):
            top = out[j * rows:j * rows + half]
            bottom = out[j * rows + half:(j + 1) * rows]
            o_ref[per * qi + j] = jnp.concatenate([top, bottom], axis=1).astype(BF16)

    n = blocks // per
    bufs = [buf_a, buf_b]
    m_old = None
    for qi in range(n + 1):
        first, second = iter(()), iter(())
        if qi < n:
            for b in range(per):
                prepare(qi * per + b)
            first = scores_of(qi, bufs[qi % 2])
        if qi:
            second = mix_of(qi - 1, bufs[(qi - 1) % 2], m_old)
        m = acc = None
        while True:
            a, b = next(first, None), next(second, None)
            if a is None and b is None:
                break
            m = m if a is None else a
            acc = acc if b is None else b
        if m is not None:
            m_old = jnp.max(m, axis=1, keepdims=True)
        if acc is not None:
            store(qi - 1, acc)


def attend(x):
    blocks = x.shape[0]
    rows = (x.shape[1] - 16) * 2 // 3
    length = blocks * rows
    return pl.pallas_call(
        attend_kernel,
        out_shape=jax.ShapeDtypeStruct((blocks, rows // 2, 128), BF16),
        in_specs=[vspec()],
        out_specs=vspec(),
        scratch_shapes=[
            pltpu.VMEM((length, 128), BF16),
            pltpu.VMEM((length, 128), BF16),
            pltpu.VMEM((length, 128), BF16),
            pltpu.VMEM((TILE, length), F32),
            pltpu.VMEM((TILE, length), F32),
        ],
        compiler_params=vmem(44),
        cost_estimate=pl.CostEstimate(
            flops=4 * length * length * 64, transcendentals=length * length // 2, bytes_accessed=4000000),
        name="attend",
    )(x)


def route_kernel(r_ref, gs_ref, es_ref, p_ref, c_ref):
    rows = r_ref.shape[0]
    experts = p_ref.shape[0] // SLOTS
    e0, e1 = r_ref[:, 0:1], r_ref[:, 1:2]
    lane = lax.broadcasted_iota(jnp.int32, (rows, 128), 1)
    named = jnp.where((lane == e0) | (lane == e1), 1.0, 0.0)
    ri = lax.broadcasted_iota(jnp.int32, (rows, rows), 0)
    ci = lax.broadcasted_iota(jnp.int32, (rows, rows), 1)
    before = jnp.where(ci < ri, 1.0, 0.0).astype(BF16)
    rank = jnp.dot(before, named.astype(BF16), preferred_element_type=F32)
    by_expert = jnp.where(named > 0, rank, -1.0).T
    slot_row = lax.broadcasted_iota(jnp.int32, (SLOTS, rows), 0).astype(F32)
    for e in range(experts):
        p_ref[e * SLOTS:(e + 1) * SLOTS, :] = jnp.where(
            by_expert[e:e + 1, :] == slot_row, 1.0, 0.0).astype(BF16)
    share = jnp.sum(jnp.where(ri == ci, gs_ref[...], 0.0), axis=1, keepdims=True)
    s0, s1 = es_ref[:, 0:1], es_ref[:, 1:2]
    total = s0 + s1
    w0, w1 = share * s0 / total, share * s1 / total
    k0 = jnp.sum(jnp.where(lane == e0, rank, 0.0), axis=1, keepdims=True).astype(jnp.int32)
    k1 = jnp.sum(jnp.where(lane == e1, rank, 0.0), axis=1, keepdims=True).astype(jnp.int32)
    at = lax.broadcasted_iota(jnp.int32, (rows, experts * SLOTS), 1)
    w = jnp.where(at == e0 * SLOTS + k0, w0, jnp.where(at == e1 * SLOTS + k1, w1, 0.0))
    hi = w.astype(BF16)
    c_ref[0:rows, :] = hi
    c_ref[rows:2 * rows, :] = (w - hi.astype(F32)).astype(BF16)


def route_tables(routes, group_share, expert_share, experts):
    rows = routes.shape[0]
    n = experts * SLOTS
    return pl.pallas_call(
        route_kernel,
        out_shape=(jax.ShapeDtypeStruct((n, rows), BF16), jax.ShapeDtypeStruct((2 * rows, n), BF16)),
        in_specs=[vspec()] * 3,
        out_specs=(vspec(),) * 2,
        compiler_params=vmem(24),
        name="route_tables",
    )(routes, group_share, expert_share)


def aspec():
    return pl.BlockSpec(memory_space=pl.ANY)


def project_kernel(*refs):
    shards = len(refs) - 15
    here_ref, a_ref = refs[0:2]
    w_refs = refs[2:2 + shards]
    res_ref, mg_ref, rg_ref, p_ref, hid_ref, out_ref = refs[2 + shards:8 + shards]
    w_scr, res_scr, mix_scr, out_scr, w_sem, r_sem, o_sem = refs[8 + shards:]
    heads, half = a_ref.shape[0], a_ref.shape[1]
    cols = w_scr.shape[2]
    loads = [pltpu.make_async_copy(w_refs[i], w_scr.at[i], w_sem.at[i]) for i in range(shards)]
    for c in loads:
        c.start()
    res_load = pltpu.make_async_copy(res_ref, res_scr, r_sem)
    res_load.start()
    tops, bottoms = [], []
    for pair in range(heads // 2):
        a = a_ref[2 * pair]
        b = a_ref[2 * pair + 1]
        tops.append(jnp.concatenate([a[:, 0:64], b[:, 0:64]], axis=1))
        bottoms.append(jnp.concatenate([a[:, 64:128], b[:, 64:128]], axis=1))
    att = jnp.concatenate([jnp.concatenate(tops, axis=1), jnp.concatenate(bottoms, axis=1)], axis=0)
    chips = shards // 2
    chip, core = lax.div(here_ref[0], 2), lax.rem(here_ref[0], 2)
    for i in range(shards):
        loads[i].wait()
        turn, swapped = i % chips, i // chips
        shard = lax.rem(chip + chips - turn, chips) * 2 + (1 - core if swapped else core)
        at = pl.multiple_of(shard * cols, cols)
        mix_scr[:, pl.ds(at, cols)] = jnp.dot(att, w_scr[i], preferred_element_type=F32)
    mixed = mix_scr[...]
    scale = lax.rsqrt(jnp.mean(mixed * mixed, axis=1, keepdims=True) + 1e-6)
    res_load.wait()
    hidden = (res_scr[...].astype(F32) + mixed * scale * mg_ref[...]).astype(BF16)
    hid_ref[...] = hidden
    h = hidden.astype(F32)
    routed = (h * lax.rsqrt(jnp.mean(h * h, axis=1, keepdims=True) + 1e-6) * rg_ref[...]).astype(BF16)
    groups = o_sem.shape[0]
    step = out_scr.shape[0] // groups
    stores = []
    for g in range(groups):
        at = slice(g * step, (g + 1) * step)
        out_scr[at, :] = jnp.dot(p_ref[at, :], routed, preferred_element_type=F32).astype(BF16)
        stores.append(pltpu.make_async_copy(out_scr.at[at], out_ref.at[at], o_sem.at[g]))
        stores[-1].start()
    for c in stores:
        c.wait()


def project(here, att, weights, residual, mix_gain, route_gain, table):
    rows, width = residual.shape
    n = len(weights)
    return pl.pallas_call(
        project_kernel,
        out_shape=(
            jax.ShapeDtypeStruct((rows, width), BF16),
            jax.ShapeDtypeStruct((table.shape[0], width), BF16),
        ),
        in_specs=[pl.BlockSpec(memory_space=pltpu.SMEM), vspec()]
        + [aspec()] * n + [aspec(), vspec(), vspec(), vspec()],
        out_specs=(vspec(), aspec()),
        scratch_shapes=[
            pltpu.VMEM((n,) + weights[0].shape, BF16),
            pltpu.VMEM((rows, width), BF16),
            pltpu.VMEM((rows, width), F32),
            pltpu.VMEM((table.shape[0], width), BF16),
            pltpu.SemaphoreType.DMA((n,)),
            pltpu.SemaphoreType.DMA,
            pltpu.SemaphoreType.DMA((4,)),
        ],
        compiler_params=vmem(36),
        name="project",
    )(here, att, *weights, residual, mix_gain, route_gain, table)


def expert_kernel(x_ref, g_ref, u_ref, d_ref, o_ref, x_scr, g_scr, u_scr, d_scr, act_scr, o_scr,
                  x_sem, g_sem, u_sem, d_sem, o_sem):
    nf, nd = g_sem.shape[0], d_sem.shape[0]
    ft, dt = g_scr.shape[2], d_scr.shape[2]

    def gate_load(f):
        return pltpu.make_async_copy(
            g_ref.at[:, pl.ds(pl.multiple_of(f * ft, ft), ft)], g_scr.at[f], g_sem.at[f])

    def up_load(f):
        return pltpu.make_async_copy(
            u_ref.at[:, pl.ds(pl.multiple_of(f * ft, ft), ft)], u_scr.at[f], u_sem.at[f])

    def down_load(j):
        return pltpu.make_async_copy(
            d_ref.at[:, pl.ds(pl.multiple_of(j * dt, dt), dt)], d_scr.at[j], d_sem.at[j])

    def out_store(j):
        return pltpu.make_async_copy(
            o_scr.at[j], o_ref.at[:, pl.ds(pl.multiple_of(j * dt, dt), dt)], o_sem.at[j])

    x_load = pltpu.make_async_copy(x_ref, x_scr, x_sem)
    gate_load(0).start()
    x_load.start()
    up_load(0).start()
    for f in range(1, nf):
        gate_load(f).start()
        up_load(f).start()
    for j in range(nd):
        down_load(j).start()
    x_load.wait()

    def hidden(f, _):
        gate_load(f).wait()
        up_load(f).wait()
        x = x_scr[...]
        gate = jnp.dot(x, g_scr[f], preferred_element_type=F32)
        upper = jnp.dot(x, u_scr[f], preferred_element_type=F32)
        act_scr[:, pl.ds(pl.multiple_of(f * ft, ft), ft)] = (
            gate / (1.0 + jnp.exp(-gate)) * upper).astype(BF16)
        return 0

    lax.fori_loop(0, nf, hidden, 0)

    def result(j, _):
        down_load(j).wait()
        o_scr[j] = jnp.dot(act_scr[...], d_scr[j], preferred_element_type=F32).astype(BF16)
        out_store(j).start()
        return 0

    lax.fori_loop(0, nd, result, 0)
    for j in range(nd):
        out_store(j).wait()


def expert(x, gate, up, down, ft=256, dt=512):
    rows, width = x.shape
    ff = gate.shape[1]
    nf, nd = ff // ft, width // dt
    return pl.pallas_call(
        expert_kernel,
        out_shape=jax.ShapeDtypeStruct((rows, width), BF16),
        in_specs=[aspec()] * 4,
        out_specs=aspec(),
        scratch_shapes=[
            pltpu.VMEM((rows, width), BF16),
            pltpu.VMEM((nf, width, ft), BF16),
            pltpu.VMEM((nf, width, ft), BF16),
            pltpu.VMEM((nd, ff, dt), BF16),
            pltpu.VMEM((rows, ff), BF16),
            pltpu.VMEM((nd, rows, dt), BF16),
            pltpu.SemaphoreType.DMA,
            pltpu.SemaphoreType.DMA((nf,)),
            pltpu.SemaphoreType.DMA((nf,)),
            pltpu.SemaphoreType.DMA((nd,)),
            pltpu.SemaphoreType.DMA((nd,)),
        ],
        compiler_params=vmem(44),
        cost_estimate=pl.CostEstimate(
            flops=6 * rows * width * ff, transcendentals=rows * ff, bytes_accessed=20000000),
        name="expert",
    )(x, gate, up, down)


def finish_kernel(c_ref, x_ref, hid_ref, og_ref, o_ref, x_scr, o_scr, x_sem, o_sem):
    rows = hid_ref.shape[0]
    n, _, ct = x_scr.shape
    loads = [
        pltpu.make_async_copy(x_ref.at[:, j * ct:(j + 1) * ct], x_scr.at[j], x_sem.at[j])
        for j in range(n)
    ]
    stores = [
        pltpu.make_async_copy(o_scr.at[j], o_ref.at[:, j * ct:(j + 1) * ct], o_sem.at[j])
        for j in range(n)
    ]
    for c in loads:
        c.start()
    for j in range(n):
        at = slice(j * ct, (j + 1) * ct)
        loads[j].wait()
        both = jnp.dot(c_ref[...], x_scr[j], preferred_element_type=F32)
        combined = both[:rows] + both[rows:]
        o_scr[j] = (hid_ref[:, at].astype(F32) + combined * og_ref[:, at]).astype(BF16)
        stores[j].start()
    for c in stores:
        c.wait()


def finish(table, x, hidden, out_gain, ct=512):
    rows, width = hidden.shape
    n = width // ct
    return pl.pallas_call(
        finish_kernel,
        out_shape=jax.ShapeDtypeStruct(hidden.shape, BF16),
        in_specs=[vspec(), aspec(), vspec(), vspec()],
        out_specs=aspec(),
        scratch_shapes=[
            pltpu.VMEM((n, x.shape[0], ct), BF16),
            pltpu.VMEM((n, rows, ct), BF16),
            pltpu.SemaphoreType.DMA((n,)),
            pltpu.SemaphoreType.DMA((n,)),
        ],
        compiler_params=vmem(24),
        name="finish",
    )(table, x, hidden, out_gain)


def swap(x):
    return lax.all_to_all(x, "sp", split_axis=0, concat_axis=0, tiled=True)


def gather_shards(x):
    n = lax.axis_size("dp")
    chips = n // 2
    own = [x]
    for k in range(1, chips):
        own.append(lax.ppermute(x, "dp", [(d, (d // 2 + k) % chips * 2 + d % 2) for d in range(n)]))
    other = [lax.ppermute(t, "dp", [(d, d ^ 1) for d in range(n)]) for t in own]
    return own + other, lax.axis_index("dp").astype(jnp.int32)[None]


def body(
    residual,
    queries,
    key_vectors,
    value_vectors,
    gate_cache,
    out_weight,
    mix_gain,
    route_gain,
    out_gain,
    routes,
    group_share,
    expert_share,
    gate_proj,
    up_proj,
    down_proj,
):
    experts = lax.axis_size("sp")
    width = residual.shape[2]
    weights, here = gather_shards(out_weight)
    arrived = swap(pack(queries[0], key_vectors[0], value_vectors[0], gate_cache[0]))
    table, back = route_tables(routes[0], group_share, expert_share[0], experts)
    att = swap(attend(arrived))
    hidden, rows_out = project(
        here, att, weights, residual[0], mix_gain[None], route_gain[None], table)

    def exchange(x):
        return swap(x.reshape(experts, SLOTS, width)).reshape(x.shape)

    result = expert(exchange(rows_out), gate_proj[0], up_proj[0], down_proj[0])
    return finish(back, exchange(result), hidden, out_gain[None])[None]


def solution(mesh):
    placed = (
        P("dp", "sp", None),
        P("dp", "sp", None),
        P("dp", "sp", None),
        P("dp", "sp", None),
        P("dp", "sp", None),
        P(None, "dp"),
        P(),
        P(),
        P(),
        P("dp", "sp", None),
        P("dp", "sp"),
        P("dp", "sp", None),
        P("sp", None, None),
        P("sp", None, None),
        P("sp", None, None),
    )
    return jax.shard_map(
        body, mesh=mesh, in_specs=placed, out_specs=P("dp", "sp", None), check_vma=False
    )
```

```python
import jax
import jax.numpy as jnp
from jax import lax
from jax.experimental import pallas as pl
from jax.experimental.pallas import tpu as pltpu
from jax.sharding import PartitionSpec as P


F32 = jnp.float32
BF16 = jnp.bfloat16
HD = 64
SLOTS = 64
NEG = -1e30


def vmem(mib):
    return pltpu.CompilerParams(vmem_limit_bytes=mib * 1024 * 1024)


def vspec():
    return pl.BlockSpec(memory_space=pltpu.VMEM)


def hspec():
    return pl.BlockSpec(memory_space=pltpu.HBM)


def pack_kernel(q_hbm, k_hbm, v_hbm, g_ref, o_hbm, q_ref, k_ref, v_ref, o_ref, in_sem, out_sem):
    rows = q_ref.shape[0]
    half = rows // 2
    heads = g_ref.shape[0]
    groups = out_sem.shape[0]
    step = heads // groups
    loads = []
    for part in range(2):
        for i, (src, dst) in enumerate(((q_hbm, q_ref), (k_hbm, k_ref), (v_hbm, v_ref))):
            cols = slice(512 * part, 512 * part + 512)
            loads.append(pltpu.make_async_copy(
                src.at[0, :, cols], dst.at[:, cols], in_sem.at[3 * part + i]))
            loads[-1].start()
    gates = g_ref[...]
    hi = gates.astype(BF16).astype(F32)
    mid = (gates - hi).astype(BF16).astype(F32)
    low = gates - hi - mid
    stores = []
    for pair in range(heads // 2):
        if pair % 4 == 0:
            for c in loads[3 * (pair // 4):3 * (pair // 4) + 3]:
                c.wait()
        cols = slice(128 * pair, 128 * pair + 128)
        q, k, v = q_ref[:, cols], k_ref[:, cols], v_ref[:, cols]
        for side in range(2):
            h = 2 * pair + side
            at = slice(64 * side, 64 * side + 64)
            o_ref[h, 0:rows, :] = jnp.concatenate([q[:, at], k[:, at]], axis=1)
            o_ref[h, rows:rows + half, :] = jnp.concatenate([v[:half, at], v[half:, at]], axis=1)
            terms = [t[h:h + 1, 128 * j:128 * j + 128] for t in (hi, mid, low) for j in range(2)]
            terms.append(jnp.zeros((10, 128), F32))
            o_ref[h, rows + half:rows + half + 16, :] = jnp.concatenate(terms, axis=0).astype(BF16)
        if (2 * pair + 2) % step == 0:
            g = (2 * pair + 2) // step - 1
            at = slice(g * step, (g + 1) * step)
            stores.append(pltpu.make_async_copy(o_ref.at[at], o_hbm.at[at], out_sem.at[g]))
            stores[-1].start()
    for c in stores:
        c.wait()


def pack(q, k, v, g):
    heads, rows = g.shape
    shape = (heads, rows + rows // 2 + 16, 128)
    return pl.pallas_call(
        pack_kernel,
        out_shape=jax.ShapeDtypeStruct(shape, BF16),
        in_specs=[hspec()] * 3 + [vspec()],
        out_specs=hspec(),
        scratch_shapes=[pltpu.VMEM(q.shape[1:], BF16)] * 3 + [
            pltpu.VMEM(shape, BF16),
            pltpu.SemaphoreType.DMA((6,)),
            pltpu.SemaphoreType.DMA((4,)),
        ],
        compiler_params=vmem(63),
        name="pack",
    )(q, k, v, g)


TILE = 512


def attend_kernel(x_ref, o_hbm, q_scr, k_scr, v_scr, buf_a, buf_b, o_ref, o_sem):
    blocks = x_ref.shape[0]
    rows = (x_ref.shape[1] - 16) * 2 // 3
    half = rows // 2
    lane = lax.broadcasted_iota(jnp.int32, (rows, 64), 1)
    minus = jnp.where(lane < 3, -1.0, 0.0).astype(BF16)
    ones = jnp.where(lane < 1, 1.0, 0.0).astype(BF16)
    pr = lax.broadcasted_iota(jnp.int32, (16, 128), 0)
    pc = lax.broadcasted_iota(jnp.int32, (16, 128), 1)
    picks = [
        jnp.where((pr == 2 * (pc - 64) + j) & (pc >= 64) & (pc < 67), 1.0, 0.0).astype(BF16)
        for j in range(2)
    ]
    nt = (((1,), (1,)), ((), ()))
    tn = (((0,), (0,)), ((), ()))

    def prepare(b):
        base = b * rows
        qk = x_ref[b, 0:rows, :]
        q = (qk[:, 0:64].astype(F32) * (HD ** -0.5)).astype(BF16)
        q_scr[base:base + rows, :] = jnp.concatenate([q, minus], axis=1)
        terms = x_ref[b, rows + half:rows + half + 16, :]
        for j in range(2):
            ext = lax.dot_general(terms, picks[j], tn, preferred_element_type=F32).astype(BF16)
            at = slice(half * j, half * j + half)
            k_scr[base + half * j:base + half * j + half, :] = jnp.concatenate(
                [qk[at, 64:128], ext[:, 64:128]], axis=1)
        v = x_ref[b, rows:rows + half, :]
        v_scr[base:base + half, :] = jnp.concatenate([v[:, 0:64], ones[:half]], axis=1)
        v_scr[base + half:base + rows, :] = jnp.concatenate([v[:, 64:128], ones[:half]], axis=1)

    def score(q0, qn, k0, kn):
        return lax.dot_general(
            q_scr[q0:q0 + qn, :], k_scr[k0:k0 + kn, :], nt, preferred_element_type=F32)

    def top_of(s, m=None):
        for j in range(s.shape[1] // 128):
            t = s[:, 128 * j:128 * j + 128]
            m = t if m is None else jnp.maximum(m, t)
        return m

    def masked(s, off):
        r = lax.broadcasted_iota(jnp.int32, s.shape, 0) + off
        c = lax.broadcasted_iota(jnp.int32, s.shape, 1)
        return jnp.where(c <= r, s, NEG)

    hq = TILE // 2

    def scores_of(qi, buf):
        q0, m = qi * TILE, None
        for k0 in range(0, q0, TILE):
            s = score(q0, TILE, k0, TILE)
            buf[:, k0:k0 + TILE] = s
            m = top_of(s, m)
            yield m
        s1 = masked(score(q0, hq, q0, hq), 0)
        s2 = masked(score(q0 + hq, hq, q0, TILE), hq)
        buf[0:hq, q0:q0 + hq] = s1
        buf[hq:TILE, q0:q0 + TILE] = s2
        d = jnp.concatenate([top_of(s1), top_of(s2)], axis=0)
        yield d if m is None else jnp.maximum(m, d)

    def mix_of(qi, buf, m):
        q0 = qi * TILE
        acc = jnp.zeros((TILE, 128), F32)
        for k0 in range(0, q0, TILE):
            p = jnp.exp(buf[:, k0:k0 + TILE] - m).astype(BF16)
            acc = acc + jnp.dot(p, v_scr[k0:k0 + TILE, :], preferred_element_type=F32)
            yield acc
        p1 = jnp.exp(buf[0:hq, q0:q0 + hq] - m[0:hq]).astype(BF16)
        p2 = jnp.exp(buf[hq:TILE, q0:q0 + TILE] - m[hq:]).astype(BF16)
        a1 = jnp.dot(p1, v_scr[q0:q0 + hq, :], preferred_element_type=F32)
        a2 = jnp.dot(p2, v_scr[q0:q0 + TILE, :], preferred_element_type=F32)
        yield acc + jnp.concatenate([a1, a2], axis=0)

    per = TILE // rows

    def store(qi, acc):
        out = acc[:, 0:64] * (1.0 / acc[:, 64:65])
        for j in range(per):
            top = out[j * rows:j * rows + half]
            bottom = out[j * rows + half:(j + 1) * rows]
            o_ref[per * qi + j] = jnp.concatenate([top, bottom], axis=1).astype(BF16)
        at = slice(per * qi, per * qi + per)
        stores.append(pltpu.make_async_copy(o_ref.at[at], o_hbm.at[at], o_sem.at[qi]))
        stores[-1].start()

    stores = []
    n = blocks // per
    bufs = [buf_a, buf_b]
    m_old = None
    for qi in range(n + 1):
        first, second = iter(()), iter(())
        if qi < n:
            for b in range(per):
                prepare(qi * per + b)
            first = scores_of(qi, bufs[qi % 2])
        if qi:
            second = mix_of(qi - 1, bufs[(qi - 1) % 2], m_old)
        m = acc = None
        while True:
            a, b = next(first, None), next(second, None)
            if a is None and b is None:
                break
            m = m if a is None else a
            acc = acc if b is None else b
        if m is not None:
            m_old = jnp.max(m, axis=1, keepdims=True)
        if acc is not None:
            store(qi - 1, acc)
    for c in stores:
        c.wait()


def attend(x):
    blocks = x.shape[0]
    rows = (x.shape[1] - 16) * 2 // 3
    length = blocks * rows
    return pl.pallas_call(
        attend_kernel,
        out_shape=jax.ShapeDtypeStruct((blocks, rows // 2, 128), BF16),
        in_specs=[vspec()],
        out_specs=hspec(),
        scratch_shapes=[
            pltpu.VMEM((length, 128), BF16),
            pltpu.VMEM((length, 128), BF16),
            pltpu.VMEM((length, 128), BF16),
            pltpu.VMEM((TILE, length), F32),
            pltpu.VMEM((TILE, length), F32),
            pltpu.VMEM((blocks, rows // 2, 128), BF16),
            pltpu.SemaphoreType.DMA((length // TILE,)),
        ],
        compiler_params=vmem(32),
        cost_estimate=pl.CostEstimate(
            flops=4 * length * length * 64, transcendentals=length * length // 2, bytes_accessed=4000000),
        name="attend",
    )(x)


def route_kernel(r_ref, gs_ref, es_ref, p_ref, c_ref):
    rows = r_ref.shape[1]
    experts = p_ref.shape[0] // SLOTS
    fill = jnp.zeros((3, rows), F32)
    columns = jnp.concatenate([r_ref[...].astype(F32), gs_ref[...], es_ref[...], fill], axis=0)
    columns = jnp.concatenate([columns, jnp.zeros((120, rows), F32)], axis=0).T
    e0, e1 = columns[:, 0:1].astype(jnp.int32), columns[:, 1:2].astype(jnp.int32)
    lane = lax.broadcasted_iota(jnp.int32, (rows, 128), 1)
    named = jnp.where((lane == e0) | (lane == e1), 1.0, 0.0)
    ri = lax.broadcasted_iota(jnp.int32, (rows, rows), 0)
    ci = lax.broadcasted_iota(jnp.int32, (rows, rows), 1)
    before = jnp.where(ci < ri, 1.0, 0.0).astype(BF16)
    rank = jnp.dot(before, named.astype(BF16), preferred_element_type=F32)
    by_expert = jnp.where(named > 0, rank, -1.0).T
    slot_row = lax.broadcasted_iota(jnp.int32, (SLOTS, rows), 0).astype(F32)
    for e in range(experts):
        p_ref[e * SLOTS:(e + 1) * SLOTS, :] = jnp.where(
            by_expert[e:e + 1, :] == slot_row, 1.0, 0.0).astype(BF16)
    share, s0, s1 = columns[:, 2:3], columns[:, 3:4], columns[:, 4:5]
    total = s0 + s1
    w0, w1 = share * s0 / total, share * s1 / total
    k0 = jnp.sum(jnp.where(lane == e0, rank, 0.0), axis=1, keepdims=True).astype(jnp.int32)
    k1 = jnp.sum(jnp.where(lane == e1, rank, 0.0), axis=1, keepdims=True).astype(jnp.int32)
    at = lax.broadcasted_iota(jnp.int32, (rows, experts * SLOTS), 1)
    w = jnp.where(at == e0 * SLOTS + k0, w0, jnp.where(at == e1 * SLOTS + k1, w1, 0.0))
    hi = w.astype(BF16)
    c_ref[0:rows, :] = hi
    c_ref[rows:2 * rows, :] = (w - hi.astype(F32)).astype(BF16)


def route_tables(routes, group_share, expert_share, experts):
    rows = routes.shape[1]
    n = experts * SLOTS
    return pl.pallas_call(
        route_kernel,
        out_shape=(jax.ShapeDtypeStruct((n, rows), BF16), jax.ShapeDtypeStruct((2 * rows, n), BF16)),
        in_specs=[vspec()] * 3,
        out_specs=(vspec(),) * 2,
        compiler_params=vmem(12),
        name="route_tables",
    )(routes, group_share, expert_share)


def project_kernel(*refs):
    shards = len(refs) - 13
    here_ref, a_ref = refs[0:2]
    w_refs = refs[2:2 + shards]
    res_ref, mg_ref, rg_ref, p_ref, hid_ref, out_ref = refs[2 + shards:8 + shards]
    w_scr, mix_scr, out_scr, w_sem, o_sem = refs[8 + shards:]
    heads, half = a_ref.shape[0], a_ref.shape[1]
    cols = w_scr.shape[2]
    loads = [pltpu.make_async_copy(w_refs[i], w_scr.at[i], w_sem.at[i]) for i in range(shards)]
    for c in loads:
        c.start()
    att = jnp.concatenate([
        jnp.concatenate([
            jnp.concatenate([a_ref[2 * j][:, side], a_ref[2 * j + 1][:, side]], axis=1)
            for j in range(heads // 2)
        ], axis=1)
        for side in (slice(0, 64), slice(64, 128))
    ], axis=0)
    chips = shards // 2
    chip, core = lax.div(here_ref[0], 2), lax.rem(here_ref[0], 2)
    for i in range(shards):
        loads[i].wait()
        turn, swapped = i % chips, i // chips
        shard = lax.rem(chip + chips - turn, chips) * 2 + (1 - core if swapped else core)
        at = pl.multiple_of(shard * cols, cols)
        mix_scr[:, pl.ds(at, cols)] = jnp.dot(att, w_scr[i], preferred_element_type=F32)
    routed = []
    for part in range(4):
        at = slice(half // 2 * part, half // 2 * (part + 1))
        mixed = mix_scr[at, :]
        scale = lax.rsqrt(jnp.mean(mixed * mixed, axis=1, keepdims=True) + 1e-6)
        hidden = (res_ref[at, :].astype(F32) + mixed * scale * mg_ref[...]).astype(BF16)
        hid_ref[at, :] = hidden
        h = hidden.astype(F32)
        scale = lax.rsqrt(jnp.mean(h * h, axis=1, keepdims=True) + 1e-6)
        routed.append((h * scale * rg_ref[...]).astype(BF16))
    routed = jnp.concatenate(routed, axis=0)
    groups = o_sem.shape[0]
    step = out_scr.shape[0] // groups
    stores = []
    for g in range(groups):
        at = slice(g * step, (g + 1) * step)
        out_scr[at, :] = jnp.dot(p_ref[at, :], routed, preferred_element_type=F32).astype(BF16)
        stores.append(pltpu.make_async_copy(out_scr.at[at], out_ref.at[at], o_sem.at[g]))
        stores[-1].start()
    for c in stores:
        c.wait()


def project(here, att, weights, residual, mix_gain, route_gain, table):
    rows, width = residual.shape
    n = len(weights)
    return pl.pallas_call(
        project_kernel,
        out_shape=(
            jax.ShapeDtypeStruct((rows, width), BF16),
            jax.ShapeDtypeStruct((table.shape[0], width), BF16),
        ),
        in_specs=[pl.BlockSpec(memory_space=pltpu.SMEM), vspec()] + [hspec()] * n + [vspec()] * 4,
        out_specs=(vspec(), hspec()),
        scratch_shapes=[
            pltpu.VMEM((n,) + weights[0].shape, BF16),
            pltpu.VMEM((rows, width), F32),
            pltpu.VMEM((table.shape[0], width), BF16),
            pltpu.SemaphoreType.DMA((n,)),
            pltpu.SemaphoreType.DMA((4,)),
        ],
        compiler_params=vmem(40),
        name="project",
    )(here, att, *weights, residual, mix_gain, route_gain, table)


def expert_kernel(x_ref, g_ref, u_ref, d_ref, o_ref, g_scr, u_scr, d_scr, act_scr, o_scr,
                  g_sem, u_sem, d_sem, o_sem):
    nf, nd = g_sem.shape[0], d_sem.shape[0]
    ft, dt = g_scr.shape[2], d_scr.shape[2]
    rows = x_ref.shape[0]
    rt = rows // 2

    def gate_load(f):
        return pltpu.make_async_copy(
            g_ref.at[:, pl.ds(pl.multiple_of(f * ft, ft), ft)], g_scr.at[f], g_sem.at[f])

    def up_load(f):
        return pltpu.make_async_copy(
            u_ref.at[:, pl.ds(pl.multiple_of(f * ft, ft), ft)], u_scr.at[f], u_sem.at[f])

    def down_load(j):
        return pltpu.make_async_copy(
            d_ref.at[:, pl.ds(pl.multiple_of(j * dt, dt), dt)], d_scr.at[j], d_sem.at[j])

    def out_store(j):
        return pltpu.make_async_copy(
            o_scr.at[j], o_ref.at[:, pl.ds(pl.multiple_of(j * dt, dt), dt)], o_sem.at[j])

    for f in range(nf):
        gate_load(f).start()
        up_load(f).start()
    for j in range(nd):
        down_load(j).start()

    def hidden(f, _):
        gate_load(f).wait()
        up_load(f).wait()
        for r in range(0, rows, rt):
            x = x_ref[r:r + rt, :]
            gate = jnp.dot(x, g_scr[f], preferred_element_type=F32)
            upper = jnp.dot(x, u_scr[f], preferred_element_type=F32)
            act_scr[r:r + rt, pl.ds(pl.multiple_of(f * ft, ft), ft)] = (
                gate / (1.0 + jnp.exp(-gate)) * upper).astype(BF16)
        return 0

    lax.fori_loop(0, nf, hidden, 0)

    def result(j, _):
        down_load(j).wait()
        o_scr[j] = jnp.dot(act_scr[...], d_scr[j], preferred_element_type=F32).astype(BF16)
        out_store(j).start()
        return 0

    lax.fori_loop(0, nd, result, 0)
    for j in range(nd):
        out_store(j).wait()


def expert(x, gate, up, down, ft=256, dt=512):
    rows, width = x.shape
    ff = gate.shape[1]
    nf, nd = ff // ft, width // dt
    return pl.pallas_call(
        expert_kernel,
        out_shape=jax.ShapeDtypeStruct((rows, width), BF16),
        in_specs=[vspec()] + [hspec()] * 3,
        out_specs=hspec(),
        scratch_shapes=[
            pltpu.VMEM((nf, width, ft), BF16),
            pltpu.VMEM((nf, width, ft), BF16),
            pltpu.VMEM((nd, ff, dt), BF16),
            pltpu.VMEM((rows, ff), BF16),
            pltpu.VMEM((nd, rows, dt), BF16),
            pltpu.SemaphoreType.DMA((nf,)),
            pltpu.SemaphoreType.DMA((nf,)),
            pltpu.SemaphoreType.DMA((nd,)),
            pltpu.SemaphoreType.DMA((nd,)),
        ],
        compiler_params=vmem(40),
        cost_estimate=pl.CostEstimate(
            flops=6 * rows * width * ff, transcendentals=rows * ff, bytes_accessed=20000000),
        name="expert",
    )(x, gate, up, down)


def finish_kernel(c_ref, x_ref, hid_ref, og_ref, o_ref, o_scr, o_sem):
    rows = hid_ref.shape[0]
    n, _, ct = o_scr.shape
    stores = [
        pltpu.make_async_copy(o_scr.at[j], o_ref.at[:, j * ct:(j + 1) * ct], o_sem.at[j])
        for j in range(n)
    ]
    for j in range(n):
        at = slice(j * ct, (j + 1) * ct)
        both = jnp.dot(c_ref[...], x_ref[:, at], preferred_element_type=F32)
        combined = both[:rows] + both[rows:]
        o_scr[j] = (hid_ref[:, at].astype(F32) + combined * og_ref[:, at]).astype(BF16)
        stores[j].start()
    for c in stores:
        c.wait()


def finish(table, x, hidden, out_gain, ct=512):
    rows, width = hidden.shape
    n = width // ct
    return pl.pallas_call(
        finish_kernel,
        out_shape=jax.ShapeDtypeStruct(hidden.shape, BF16),
        in_specs=[vspec()] * 4,
        out_specs=hspec(),
        scratch_shapes=[pltpu.VMEM((n, rows, ct), BF16), pltpu.SemaphoreType.DMA((n,))],
        compiler_params=vmem(16),
        name="finish",
    )(table, x, hidden, out_gain)


def swap(x):
    return lax.all_to_all(x, "sp", split_axis=0, concat_axis=0, tiled=True)


def gather_shards(x):
    n = lax.axis_size("dp")
    chips = n // 2
    own = [x]
    for k in range(1, chips):
        own.append(
            lax.ppermute(x, "dp", [(d, (d // 2 + k) % chips * 2 + d % 2) for d in range(n)]))
    other = [lax.ppermute(t, "dp", [(d, d ^ 1) for d in range(n)]) for t in own]
    return own + other, lax.axis_index("dp").astype(jnp.int32)[None]


def layer(
    residual,
    queries,
    key_vectors,
    value_vectors,
    gate_cache,
    out_weight,
    mix_gain,
    route_gain,
    out_gain,
    routes,
    group_share,
    expert_share,
    gate_proj,
    up_proj,
    down_proj,
):
    experts = lax.axis_size("sp")
    width = residual.shape[2]
    weights, here = gather_shards(out_weight)
    packed = pack(queries, key_vectors, value_vectors, gate_cache[0].T)
    arrived = swap(packed)
    table, back = route_tables(routes[0].T, group_share, expert_share[0].T, experts)
    attended = attend(arrived)
    att = swap(attended)
    hidden, rows_out = project(
        here, att, weights, residual[0], mix_gain[None], route_gain[None], table)

    def exchange(x):
        return swap(x.reshape(experts, SLOTS, width)).reshape(x.shape)

    result = expert(exchange(rows_out), gate_proj[0], up_proj[0], down_proj[0])
    return finish(back, exchange(result), hidden, out_gain[None])[None]


def solution(mesh):
    placed = (
        P("dp", "sp", None),
        P("dp", "sp", None),
        P("dp", "sp", None),
        P("dp", "sp", None),
        P("dp", "sp", None),
        P(None, "dp"),
        P(),
        P(),
        P(),
        P("dp", "sp", None),
        P("dp", "sp"),
        P("dp", "sp", None),
        P("sp", None, None),
        P("sp", None, None),
        P("sp", None, None),
    )
    return jax.shard_map(
        layer, mesh=mesh, in_specs=placed, out_specs=P("dp", "sp", None), check_vma=False
    )
```

```python
import jax
import jax.numpy as jnp
from jax import lax
from jax.experimental import pallas as pl
from jax.experimental.pallas import tpu as pltpu
from jax.sharding import PartitionSpec as P


F32 = jnp.float32
BF16 = jnp.bfloat16
HD = 64
SLOTS = 64
NEG = -1e30


def vmem(mib):
    return pltpu.CompilerParams(vmem_limit_bytes=mib * 1024 * 1024)


def vspec():
    return pl.BlockSpec(memory_space=pltpu.VMEM)


def hspec():
    return pl.BlockSpec(memory_space=pltpu.HBM)


def pack_kernel(q_hbm, k_hbm, v_hbm, g_ref, o_hbm, q_ref, k_ref, v_ref, o_ref, in_sem, out_sem):
    rows = q_ref.shape[0]
    half = rows // 2
    heads = g_ref.shape[0]
    groups = out_sem.shape[0]
    step = heads // groups
    loads = []
    for part in range(2):
        for i, (src, dst) in enumerate(((q_hbm, q_ref), (k_hbm, k_ref), (v_hbm, v_ref))):
            cols = slice(512 * part, 512 * part + 512)
            loads.append(pltpu.make_async_copy(
                src.at[0, :, cols], dst.at[:, cols], in_sem.at[3 * part + i]))
            loads[-1].start()
    gates = g_ref[...]
    hi = gates.astype(BF16).astype(F32)
    mid = (gates - hi).astype(BF16).astype(F32)
    low = gates - hi - mid
    stores = []
    for pair in range(heads // 2):
        if pair % 4 == 0:
            for c in loads[3 * (pair // 4):3 * (pair // 4) + 3]:
                c.wait()
        cols = slice(128 * pair, 128 * pair + 128)
        q, k, v = q_ref[:, cols], k_ref[:, cols], v_ref[:, cols]
        for side in range(2):
            h = 2 * pair + side
            at = slice(64 * side, 64 * side + 64)
            o_ref[h, 0:rows, :] = jnp.concatenate([q[:, at], k[:, at]], axis=1)
            o_ref[h, rows:rows + half, :] = jnp.concatenate([v[:half, at], v[half:, at]], axis=1)
            terms = [t[h:h + 1, 128 * j:128 * j + 128] for t in (hi, mid, low) for j in range(2)]
            terms.append(jnp.zeros((10, 128), F32))
            o_ref[h, rows + half:rows + half + 16, :] = jnp.concatenate(terms, axis=0).astype(BF16)
        if (2 * pair + 2) % step == 0:
            g = (2 * pair + 2) // step - 1
            at = slice(g * step, (g + 1) * step)
            stores.append(pltpu.make_async_copy(o_ref.at[at], o_hbm.at[at], out_sem.at[g]))
            stores[-1].start()
    for c in stores:
        c.wait()


def pack(q, k, v, g):
    heads, rows = g.shape
    shape = (heads, rows + rows // 2 + 16, 128)
    return pl.pallas_call(
        pack_kernel,
        out_shape=jax.ShapeDtypeStruct(shape, BF16),
        in_specs=[hspec()] * 3 + [vspec()],
        out_specs=hspec(),
        scratch_shapes=[pltpu.VMEM(q.shape[1:], BF16)] * 3 + [
            pltpu.VMEM(shape, BF16),
            pltpu.SemaphoreType.DMA((6,)),
            pltpu.SemaphoreType.DMA((4,)),
        ],
        compiler_params=vmem(63),
        name="pack",
    )(q, k, v, g)


TILE = 512


def attend_kernel(x_hbm, o_hbm, q_scr, k_scr, v_scr, buf_a, buf_b, x_ref, o_ref, x_sem, o_sem):
    blocks = x_ref.shape[0]
    rows = (x_ref.shape[1] - 16) * 2 // 3
    half = rows // 2
    per = TILE // rows
    loads = []
    for i in range(blocks // per):
        at = slice(per * i, per * i + per)
        loads.append(pltpu.make_async_copy(x_hbm.at[at], x_ref.at[at], x_sem.at[i]))
        loads[-1].start()
    lane = lax.broadcasted_iota(jnp.int32, (rows, 64), 1)
    minus = jnp.where(lane < 3, -1.0, 0.0).astype(BF16)
    ones = jnp.where(lane < 1, 1.0, 0.0).astype(BF16)
    pr = lax.broadcasted_iota(jnp.int32, (16, 128), 0)
    pc = lax.broadcasted_iota(jnp.int32, (16, 128), 1)
    picks = [
        jnp.where((pr == 2 * (pc - 64) + j) & (pc >= 64) & (pc < 67), 1.0, 0.0).astype(BF16)
        for j in range(2)
    ]
    nt = (((1,), (1,)), ((), ()))
    tn = (((0,), (0,)), ((), ()))

    def prepare(b):
        base = b * rows
        qk = x_ref[b, 0:rows, :]
        q = (qk[:, 0:64].astype(F32) * (HD ** -0.5)).astype(BF16)
        q_scr[base:base + rows, :] = jnp.concatenate([q, minus], axis=1)
        terms = x_ref[b, rows + half:rows + half + 16, :]
        for j in range(2):
            ext = lax.dot_general(terms, picks[j], tn, preferred_element_type=F32).astype(BF16)
            at = slice(half * j, half * j + half)
            k_scr[base + half * j:base + half * j + half, :] = jnp.concatenate(
                [qk[at, 64:128], ext[:, 64:128]], axis=1)
        v = x_ref[b, rows:rows + half, :]
        v_scr[base:base + half, :] = jnp.concatenate([v[:, 0:64], ones[:half]], axis=1)
        v_scr[base + half:base + rows, :] = jnp.concatenate([v[:, 64:128], ones[:half]], axis=1)

    def score(q0, qn, k0, kn):
        return lax.dot_general(
            q_scr[q0:q0 + qn, :], k_scr[k0:k0 + kn, :], nt, preferred_element_type=F32)

    def top_of(s, m=None):
        for j in range(s.shape[1] // 128):
            t = s[:, 128 * j:128 * j + 128]
            m = t if m is None else jnp.maximum(m, t)
        return m

    def masked(s, off):
        r = lax.broadcasted_iota(jnp.int32, s.shape, 0) + off
        c = lax.broadcasted_iota(jnp.int32, s.shape, 1)
        return jnp.where(c <= r, s, NEG)

    hq = TILE // 2

    def scores_of(qi, buf):
        q0, m = qi * TILE, None
        for k0 in range(0, q0, TILE):
            s = score(q0, TILE, k0, TILE)
            buf[:, k0:k0 + TILE] = s
            m = top_of(s, m)
            yield m
        s1 = masked(score(q0, hq, q0, hq), 0)
        s2 = masked(score(q0 + hq, hq, q0, TILE), hq)
        buf[0:hq, q0:q0 + hq] = s1
        buf[hq:TILE, q0:q0 + TILE] = s2
        d = jnp.concatenate([top_of(s1), top_of(s2)], axis=0)
        yield d if m is None else jnp.maximum(m, d)

    def mix_of(qi, buf, m):
        q0 = qi * TILE
        acc = jnp.zeros((TILE, 128), F32)
        for k0 in range(0, q0, TILE):
            p = jnp.exp(buf[:, k0:k0 + TILE] - m).astype(BF16)
            acc = acc + jnp.dot(p, v_scr[k0:k0 + TILE, :], preferred_element_type=F32)
            yield acc
        p1 = jnp.exp(buf[0:hq, q0:q0 + hq] - m[0:hq]).astype(BF16)
        p2 = jnp.exp(buf[hq:TILE, q0:q0 + TILE] - m[hq:]).astype(BF16)
        a1 = jnp.dot(p1, v_scr[q0:q0 + hq, :], preferred_element_type=F32)
        a2 = jnp.dot(p2, v_scr[q0:q0 + TILE, :], preferred_element_type=F32)
        yield acc + jnp.concatenate([a1, a2], axis=0)

    def store(qi, acc):
        out = acc[:, 0:64] * (1.0 / acc[:, 64:65])
        for j in range(per):
            top = out[j * rows:j * rows + half]
            bottom = out[j * rows + half:(j + 1) * rows]
            o_ref[per * qi + j] = jnp.concatenate([top, bottom], axis=1).astype(BF16)
        at = slice(per * qi, per * qi + per)
        stores.append(pltpu.make_async_copy(o_ref.at[at], o_hbm.at[at], o_sem.at[qi]))
        stores[-1].start()

    stores = []
    n = blocks // per
    bufs = [buf_a, buf_b]
    m_old = None
    for qi in range(n + 1):
        first, second = iter(()), iter(())
        if qi < n:
            loads[qi].wait()
            for b in range(per):
                prepare(qi * per + b)
            first = scores_of(qi, bufs[qi % 2])
        if qi:
            second = mix_of(qi - 1, bufs[(qi - 1) % 2], m_old)
        m = acc = None
        while True:
            a, b = next(first, None), next(second, None)
            if a is None and b is None:
                break
            m = m if a is None else a
            acc = acc if b is None else b
        if m is not None:
            m_old = jnp.max(m, axis=1, keepdims=True)
        if acc is not None:
            store(qi - 1, acc)
    for c in stores:
        c.wait()


def attend(x):
    blocks = x.shape[0]
    rows = (x.shape[1] - 16) * 2 // 3
    length = blocks * rows
    return pl.pallas_call(
        attend_kernel,
        out_shape=jax.ShapeDtypeStruct((blocks, rows // 2, 128), BF16),
        in_specs=[hspec()],
        out_specs=hspec(),
        scratch_shapes=[
            pltpu.VMEM((length, 128), BF16),
            pltpu.VMEM((length, 128), BF16),
            pltpu.VMEM((length, 128), BF16),
            pltpu.VMEM((TILE, length), F32),
            pltpu.VMEM((TILE, length), F32),
            pltpu.VMEM(x.shape, BF16),
            pltpu.VMEM((blocks, rows // 2, 128), BF16),
            pltpu.SemaphoreType.DMA((length // TILE,)),
            pltpu.SemaphoreType.DMA((length // TILE,)),
        ],
        compiler_params=vmem(62),
        cost_estimate=pl.CostEstimate(
            flops=4 * length * length * 64, transcendentals=length * length // 2, bytes_accessed=4000000),
        name="attend",
    )(x)


def route_kernel(r_ref, gs_ref, es_ref, p_ref, c_ref):
    rows = r_ref.shape[1]
    experts = p_ref.shape[0]
    fill = jnp.zeros((3, rows), F32)
    columns = jnp.concatenate([r_ref[...].astype(F32), gs_ref[...], es_ref[...], fill], axis=0)
    columns = jnp.concatenate([columns, jnp.zeros((120, rows), F32)], axis=0).T
    e0, e1 = columns[:, 0:1].astype(jnp.int32), columns[:, 1:2].astype(jnp.int32)
    lane = lax.broadcasted_iota(jnp.int32, (rows, 128), 1)
    named = jnp.where((lane == e0) | (lane == e1), 1.0, 0.0)
    ri = lax.broadcasted_iota(jnp.int32, (rows, rows), 0)
    ci = lax.broadcasted_iota(jnp.int32, (rows, rows), 1)
    before = jnp.where(ci < ri, 1.0, 0.0).astype(BF16)
    rank = jnp.dot(before, named.astype(BF16), preferred_element_type=F32)
    p_ref[...] = jnp.where(named > 0, rank, -1.0).T[:experts]
    share, s0, s1 = columns[:, 2:3], columns[:, 3:4], columns[:, 4:5]
    total = s0 + s1
    w0, w1 = share * s0 / total, share * s1 / total
    k0 = jnp.sum(jnp.where(lane == e0, rank, 0.0), axis=1, keepdims=True).astype(jnp.int32)
    k1 = jnp.sum(jnp.where(lane == e1, rank, 0.0), axis=1, keepdims=True).astype(jnp.int32)
    at = lax.broadcasted_iota(jnp.int32, (rows, experts * SLOTS), 1)
    w = jnp.where(at == e0 * SLOTS + k0, w0, jnp.where(at == e1 * SLOTS + k1, w1, 0.0))
    c_ref[...] = w.astype(BF16)


def route_tables(routes, group_share, expert_share, experts):
    rows = routes.shape[1]
    n = experts * SLOTS
    return pl.pallas_call(
        route_kernel,
        out_shape=(jax.ShapeDtypeStruct((experts, rows), F32), jax.ShapeDtypeStruct((rows, n), BF16)),
        in_specs=[vspec()] * 3,
        out_specs=(vspec(),) * 2,
        compiler_params=vmem(12),
        name="route_tables",
    )(routes, group_share, expert_share)


def project_kernel(*refs):
    shards = len(refs) - 12
    here_ref, a_ref = refs[0:2]
    w_refs = refs[2:2 + shards]
    res_ref, mg_ref, rg_ref, p_ref, hid_ref, out_ref = refs[2 + shards:8 + shards]
    w_scr, mix_scr, p_scr, w_sem = refs[8 + shards:]
    heads, half = a_ref.shape[0], a_ref.shape[1]
    cols = w_scr.shape[2]
    loads = [pltpu.make_async_copy(w_refs[i], w_scr.at[i], w_sem.at[i]) for i in range(shards)]
    for c in loads:
        c.start()
    rows = p_ref.shape[1]
    slot = lax.broadcasted_iota(jnp.int32, (SLOTS, rows), 0).astype(F32)
    for e in range(p_ref.shape[0]):
        p_scr[e * SLOTS:(e + 1) * SLOTS, :] = jnp.where(
            p_ref[e:e + 1, :] == slot, 1.0, 0.0).astype(BF16)
    att = jnp.concatenate([
        jnp.concatenate([
            jnp.concatenate([a_ref[2 * j][:, side], a_ref[2 * j + 1][:, side]], axis=1)
            for j in range(heads // 2)
        ], axis=1)
        for side in (slice(0, 64), slice(64, 128))
    ], axis=0)
    chips = shards // 2
    chip, core = lax.div(here_ref[0], 2), lax.rem(here_ref[0], 2)
    for i in range(shards):
        loads[i].wait()
        turn, swapped = i % chips, i // chips
        shard = lax.rem(chip + chips - turn, chips) * 2 + (1 - core if swapped else core)
        at = pl.multiple_of(shard * cols, cols)
        mix_scr[:, pl.ds(at, cols)] = jnp.dot(att, w_scr[i], preferred_element_type=F32)
    width = mix_scr.shape[1]
    scales = []
    for part in range(4):
        at = slice(half // 2 * part, half // 2 * (part + 1))
        mixed = mix_scr[at, :]
        scale = lax.rsqrt(jnp.mean(mixed * mixed, axis=1, keepdims=True) + 1e-6)
        hidden = (res_ref[at, :].astype(F32) + mixed * scale * mg_ref[...]).astype(BF16)
        hid_ref[at, :] = hidden
        h = hidden.astype(F32)
        scales.append(lax.rsqrt(jnp.mean(h * h, axis=1, keepdims=True) + 1e-6))
    scale = jnp.concatenate(scales, axis=0)
    for j in range(0, width, 512):
        at = slice(j, j + 512)
        routed = (hid_ref[:, at].astype(F32) * scale * rg_ref[:, at]).astype(BF16)
        out_ref[:, at] = jnp.dot(p_scr[...], routed, preferred_element_type=F32).astype(BF16)


def project(here, att, weights, residual, mix_gain, route_gain, table):
    rows, width = residual.shape
    n = len(weights)
    return pl.pallas_call(
        project_kernel,
        out_shape=(
            jax.ShapeDtypeStruct((rows, width), BF16),
            jax.ShapeDtypeStruct((table.shape[0] * SLOTS, width), BF16),
        ),
        in_specs=[pl.BlockSpec(memory_space=pltpu.SMEM), vspec()] + [hspec()] * n + [vspec()] * 4,
        out_specs=(vspec(), vspec()),
        scratch_shapes=[
            pltpu.VMEM((n,) + weights[0].shape, BF16),
            pltpu.VMEM((rows, width), F32),
            pltpu.VMEM((table.shape[0] * SLOTS, rows), BF16),
            pltpu.SemaphoreType.DMA((n,)),
        ],
        compiler_params=vmem(40),
        name="project",
    )(here, att, *weights, residual, mix_gain, route_gain, table)


def expert_kernel(x_ref, g_ref, u_ref, d_ref, o_ref, act_scr):
    ft, dt = 512, 512

    def hidden(f, _):
        at = pl.ds(pl.multiple_of(f * ft, ft), ft)
        gate = jnp.dot(x_ref[...], g_ref[:, at], preferred_element_type=F32)
        upper = jnp.dot(x_ref[...], u_ref[:, at], preferred_element_type=F32)
        act_scr[:, at] = (gate / (1.0 + jnp.exp(-gate)) * upper).astype(BF16)
        return 0

    lax.fori_loop(0, act_scr.shape[1] // ft, hidden, 0)

    def result(j, _):
        at = pl.ds(pl.multiple_of(j * dt, dt), dt)
        o_ref[:, at] = jnp.dot(act_scr[...], d_ref[:, at], preferred_element_type=F32).astype(BF16)
        return 0

    lax.fori_loop(0, o_ref.shape[1] // dt, result, 0)


def expert(x, gate, up, down):
    rows, width = x.shape
    ff = gate.shape[1]
    return pl.pallas_call(
        expert_kernel,
        out_shape=jax.ShapeDtypeStruct((rows, width), BF16),
        in_specs=[vspec()] * 4,
        out_specs=vspec(),
        scratch_shapes=[pltpu.VMEM((rows, ff), BF16)],
        compiler_params=vmem(26),
        cost_estimate=pl.CostEstimate(
            flops=6 * rows * width * ff, transcendentals=rows * ff, bytes_accessed=20000000),
        name="expert",
    )(x, gate, up, down)


def finish_kernel(c_ref, x_ref, hid_ref, og_ref, o_ref, o_scr, o_sem):
    n, _, ct = o_scr.shape
    stores = [
        pltpu.make_async_copy(o_scr.at[j], o_ref.at[:, j * ct:(j + 1) * ct], o_sem.at[j])
        for j in range(n)
    ]
    for j in range(n):
        at = slice(j * ct, (j + 1) * ct)
        combined = jnp.dot(c_ref[...], x_ref[:, at], preferred_element_type=F32)
        o_scr[j] = (hid_ref[:, at].astype(F32) + combined * og_ref[:, at]).astype(BF16)
        stores[j].start()
    for c in stores:
        c.wait()


def finish(table, x, hidden, out_gain, ct=512):
    rows, width = hidden.shape
    n = width // ct
    return pl.pallas_call(
        finish_kernel,
        out_shape=jax.ShapeDtypeStruct(hidden.shape, BF16),
        in_specs=[vspec()] * 4,
        out_specs=hspec(),
        scratch_shapes=[pltpu.VMEM((n, rows, ct), BF16), pltpu.SemaphoreType.DMA((n,))],
        compiler_params=vmem(16),
        name="finish",
    )(table, x, hidden, out_gain)


def swap(x):
    return lax.all_to_all(x, "sp", split_axis=0, concat_axis=0, tiled=True)


def gather_shards(x):
    n = lax.axis_size("dp")
    chips = n // 2
    own = [x]
    for k in range(1, chips):
        own.append(
            lax.ppermute(x, "dp", [(d, (d // 2 + k) % chips * 2 + d % 2) for d in range(n)]))
    other = [lax.ppermute(t, "dp", [(d, d ^ 1) for d in range(n)]) for t in own]
    return own + other, lax.axis_index("dp").astype(jnp.int32)[None]


def layer(
    residual,
    queries,
    key_vectors,
    value_vectors,
    gate_cache,
    out_weight,
    mix_gain,
    route_gain,
    out_gain,
    routes,
    group_share,
    expert_share,
    gate_proj,
    up_proj,
    down_proj,
):
    experts = lax.axis_size("sp")
    width = residual.shape[2]
    weights, here = gather_shards(out_weight)
    packed = pack(queries, key_vectors, value_vectors, gate_cache[0].T)
    arrived = swap(packed)
    table, back = route_tables(routes[0].T, group_share, expert_share[0].T, experts)
    attended = attend(arrived)
    att = swap(attended)
    hidden, rows_out = project(
        here, att, weights, residual[0], mix_gain[None], route_gain[None], table)

    def exchange(x):
        return swap(x.reshape(experts, SLOTS, width)).reshape(x.shape)

    result = expert(exchange(rows_out), gate_proj[0], up_proj[0], down_proj[0])
    return finish(back, exchange(result), hidden, out_gain[None])[None]


def solution(mesh):
    placed = (
        P("dp", "sp", None),
        P("dp", "sp", None),
        P("dp", "sp", None),
        P("dp", "sp", None),
        P("dp", "sp", None),
        P(None, "dp"),
        P(),
        P(),
        P(),
        P("dp", "sp", None),
        P("dp", "sp"),
        P("dp", "sp", None),
        P("sp", None, None),
        P("sp", None, None),
        P("sp", None, None),
    )
    return jax.shard_map(
        layer, mesh=mesh, in_specs=placed, out_specs=P("dp", "sp", None), check_vma=False
    )
```

```python
import jax
import jax.numpy as jnp
from jax import lax
from jax.experimental import pallas as pl
from jax.experimental.pallas import tpu as pltpu
from jax.sharding import PartitionSpec as P


F32 = jnp.float32
BF16 = jnp.bfloat16
HD = 64
SLOTS = 64
NEG = -1e30


def vmem(mib):
    return pltpu.CompilerParams(vmem_limit_bytes=mib * 1024 * 1024)


def vspec():
    return pl.BlockSpec(memory_space=pltpu.VMEM)


def hspec():
    return pl.BlockSpec(memory_space=pltpu.HBM)


def pack_kernel(q_hbm, k_hbm, v_hbm, g_ref, o_hbm, q_ref, k_ref, v_ref, o_ref, in_sem, out_sem):
    rows = q_ref.shape[0]
    half = rows // 2
    heads = g_ref.shape[0]
    groups = out_sem.shape[0]
    step = heads // groups
    loads = []
    for part in range(2):
        for i, (src, dst) in enumerate(((q_hbm, q_ref), (k_hbm, k_ref), (v_hbm, v_ref))):
            cols = slice(512 * part, 512 * part + 512)
            loads.append(pltpu.make_async_copy(
                src.at[0, :, cols], dst.at[:, cols], in_sem.at[3 * part + i]))
            loads[-1].start()
    gates = g_ref[...]
    hi = gates.astype(BF16).astype(F32)
    mid = (gates - hi).astype(BF16).astype(F32)
    low = gates - hi - mid
    stores = []
    for pair in range(heads // 2):
        if pair % 4 == 0:
            for c in loads[3 * (pair // 4):3 * (pair // 4) + 3]:
                c.wait()
        cols = slice(128 * pair, 128 * pair + 128)
        q, k, v = q_ref[:, cols], k_ref[:, cols], v_ref[:, cols]
        for side in range(2):
            h = 2 * pair + side
            at = slice(64 * side, 64 * side + 64)
            o_ref[h, 0:rows, :] = jnp.concatenate([q[:, at], k[:, at]], axis=1)
            o_ref[h, rows:rows + half, :] = jnp.concatenate([v[:half, at], v[half:, at]], axis=1)
            terms = [t[h:h + 1, 128 * j:128 * j + 128] for t in (hi, mid, low) for j in range(2)]
            terms.append(jnp.zeros((10, 128), F32))
            o_ref[h, rows + half:rows + half + 16, :] = jnp.concatenate(terms, axis=0).astype(BF16)
        if (2 * pair + 2) % step == 0:
            g = (2 * pair + 2) // step - 1
            at = slice(g * step, (g + 1) * step)
            stores.append(pltpu.make_async_copy(o_ref.at[at], o_hbm.at[at], out_sem.at[g]))
            stores[-1].start()
    for c in stores:
        c.wait()


def pack(q, k, v, g):
    heads, rows = g.shape
    shape = (heads, rows + rows // 2 + 16, 128)
    return pl.pallas_call(
        pack_kernel,
        out_shape=jax.ShapeDtypeStruct(shape, BF16),
        in_specs=[hspec()] * 3 + [vspec()],
        out_specs=hspec(),
        scratch_shapes=[pltpu.VMEM(q.shape[1:], BF16)] * 3 + [
            pltpu.VMEM(shape, BF16),
            pltpu.SemaphoreType.DMA((6,)),
            pltpu.SemaphoreType.DMA((4,)),
        ],
        compiler_params=vmem(63),
        name="pack",
    )(q, k, v, g)


TILE = 512


def attend_kernel(x_ref, o_ref, q_scr, k_scr, v_scr, buf_a, buf_b):
    blocks = x_ref.shape[0]
    rows = (x_ref.shape[1] - 16) * 2 // 3
    half = rows // 2
    lane = lax.broadcasted_iota(jnp.int32, (rows, 64), 1)
    minus = jnp.where(lane < 3, -1.0, 0.0).astype(BF16)
    ones = jnp.where(lane < 1, 1.0, 0.0).astype(BF16)
    pr = lax.broadcasted_iota(jnp.int32, (16, 128), 0)
    pc = lax.broadcasted_iota(jnp.int32, (16, 128), 1)
    picks = [
        jnp.where((pr == 2 * (pc - 64) + j) & (pc >= 64) & (pc < 67), 1.0, 0.0).astype(BF16)
        for j in range(2)
    ]
    nt = (((1,), (1,)), ((), ()))
    tn = (((0,), (0,)), ((), ()))

    def prepare(b):
        base = b * rows
        qk = x_ref[b, 0:rows, :]
        q = (qk[:, 0:64].astype(F32) * (HD ** -0.5)).astype(BF16)
        q_scr[base:base + rows, :] = jnp.concatenate([q, minus], axis=1)
        terms = x_ref[b, rows + half:rows + half + 16, :]
        for j in range(2):
            ext = lax.dot_general(terms, picks[j], tn, preferred_element_type=F32).astype(BF16)
            at = slice(half * j, half * j + half)
            k_scr[base + half * j:base + half * j + half, :] = jnp.concatenate(
                [qk[at, 64:128], ext[:, 64:128]], axis=1)
        v = x_ref[b, rows:rows + half, :]
        v_scr[base:base + half, :] = jnp.concatenate([v[:, 0:64], ones[:half]], axis=1)
        v_scr[base + half:base + rows, :] = jnp.concatenate([v[:, 64:128], ones[:half]], axis=1)

    def score(q0, qn, k0, kn):
        return lax.dot_general(
            q_scr[q0:q0 + qn, :], k_scr[k0:k0 + kn, :], nt, preferred_element_type=F32)

    def top_of(s, m=None):
        for j in range(s.shape[1] // 128):
            t = s[:, 128 * j:128 * j + 128]
            m = t if m is None else jnp.maximum(m, t)
        return m

    def masked(s, off):
        r = lax.broadcasted_iota(jnp.int32, s.shape, 0) + off
        c = lax.broadcasted_iota(jnp.int32, s.shape, 1)
        return jnp.where(c <= r, s, NEG)

    hq = TILE // 2

    def scores_of(qi, buf):
        q0, m = qi * TILE, None
        for k0 in range(0, q0, TILE):
            s = score(q0, TILE, k0, TILE)
            buf[:, k0:k0 + TILE] = s
            m = top_of(s, m)
            yield m
        s1 = masked(score(q0, hq, q0, hq), 0)
        s2 = masked(score(q0 + hq, hq, q0, TILE), hq)
        buf[0:hq, q0:q0 + hq] = s1
        buf[hq:TILE, q0:q0 + TILE] = s2
        d = jnp.concatenate([top_of(s1), top_of(s2)], axis=0)
        yield d if m is None else jnp.maximum(m, d)

    def mix_of(qi, buf, m):
        q0 = qi * TILE
        acc = jnp.zeros((TILE, 128), F32)
        for k0 in range(0, q0, TILE):
            p = jnp.exp(buf[:, k0:k0 + TILE] - m).astype(BF16)
            acc = acc + jnp.dot(p, v_scr[k0:k0 + TILE, :], preferred_element_type=F32)
            yield acc
        p1 = jnp.exp(buf[0:hq, q0:q0 + hq] - m[0:hq]).astype(BF16)
        p2 = jnp.exp(buf[hq:TILE, q0:q0 + TILE] - m[hq:]).astype(BF16)
        a1 = jnp.dot(p1, v_scr[q0:q0 + hq, :], preferred_element_type=F32)
        a2 = jnp.dot(p2, v_scr[q0:q0 + TILE, :], preferred_element_type=F32)
        yield acc + jnp.concatenate([a1, a2], axis=0)

    per = TILE // rows

    def store(qi, acc):
        out = acc[:, 0:64] * (1.0 / acc[:, 64:65])
        for j in range(per):
            top = out[j * rows:j * rows + half]
            bottom = out[j * rows + half:(j + 1) * rows]
            o_ref[per * qi + j] = jnp.concatenate([top, bottom], axis=1).astype(BF16)

    n = blocks // per
    bufs = [buf_a, buf_b]
    m_old = None
    for qi in range(n + 1):
        first, second = iter(()), iter(())
        if qi < n:
            for b in range(per):
                prepare(qi * per + b)
            first = scores_of(qi, bufs[qi % 2])
        if qi:
            second = mix_of(qi - 1, bufs[(qi - 1) % 2], m_old)
        m = acc = None
        while True:
            a, b = next(first, None), next(second, None)
            if a is None and b is None:
                break
            m = m if a is None else a
            acc = acc if b is None else b
        if m is not None:
            m_old = jnp.max(m, axis=1, keepdims=True)
        if acc is not None:
            store(qi - 1, acc)


def attend(x):
    blocks = x.shape[0]
    rows = (x.shape[1] - 16) * 2 // 3
    length = blocks * rows
    return pl.pallas_call(
        attend_kernel,
        out_shape=jax.ShapeDtypeStruct((blocks, rows // 2, 128), BF16),
        in_specs=[vspec()],
        out_specs=vspec(),
        scratch_shapes=[
            pltpu.VMEM((length, 128), BF16),
            pltpu.VMEM((length, 128), BF16),
            pltpu.VMEM((length, 128), BF16),
            pltpu.VMEM((TILE, length), F32),
            pltpu.VMEM((TILE, length), F32),
        ],
        compiler_params=pltpu.CompilerParams(vmem_limit_bytes=54000000),
        cost_estimate=pl.CostEstimate(
            flops=4 * length * length * 64, transcendentals=length * length // 2, bytes_accessed=4000000),
        name="attend",
    )(x)


def route_kernel(r_ref, gs_ref, es_ref, p_ref, c_ref):
    rows = r_ref.shape[1]
    experts = p_ref.shape[0]
    fill = jnp.zeros((3, rows), F32)
    columns = jnp.concatenate([r_ref[...].astype(F32), gs_ref[...], es_ref[...], fill], axis=0)
    columns = jnp.concatenate([columns, jnp.zeros((120, rows), F32)], axis=0).T
    e0, e1 = columns[:, 0:1].astype(jnp.int32), columns[:, 1:2].astype(jnp.int32)
    lane = lax.broadcasted_iota(jnp.int32, (rows, 128), 1)
    named = jnp.where((lane == e0) | (lane == e1), 1.0, 0.0)
    ri = lax.broadcasted_iota(jnp.int32, (rows, rows), 0)
    ci = lax.broadcasted_iota(jnp.int32, (rows, rows), 1)
    before = jnp.where(ci < ri, 1.0, 0.0).astype(BF16)
    rank = jnp.dot(before, named.astype(BF16), preferred_element_type=F32)
    p_ref[...] = jnp.where(named > 0, rank, -1.0).T[:experts]
    share, s0, s1 = columns[:, 2:3], columns[:, 3:4], columns[:, 4:5]
    total = s0 + s1
    w0, w1 = share * s0 / total, share * s1 / total
    k0 = jnp.sum(jnp.where(lane == e0, rank, 0.0), axis=1, keepdims=True).astype(jnp.int32)
    k1 = jnp.sum(jnp.where(lane == e1, rank, 0.0), axis=1, keepdims=True).astype(jnp.int32)
    at = lax.broadcasted_iota(jnp.int32, (rows, experts * SLOTS), 1)
    w = jnp.where(at == e0 * SLOTS + k0, w0, jnp.where(at == e1 * SLOTS + k1, w1, 0.0))
    c_ref[...] = w.astype(BF16)


def route_tables(routes, group_share, expert_share, experts):
    rows = routes.shape[1]
    n = experts * SLOTS
    return pl.pallas_call(
        route_kernel,
        out_shape=(jax.ShapeDtypeStruct((experts, rows), F32), jax.ShapeDtypeStruct((rows, n), BF16)),
        in_specs=[vspec()] * 3,
        out_specs=(vspec(),) * 2,
        compiler_params=vmem(12),
        name="route_tables",
    )(routes, group_share, expert_share)


def project_kernel(*refs):
    shards = len(refs) - 12
    here_ref, a_ref = refs[0:2]
    w_refs = refs[2:2 + shards]
    res_ref, mg_ref, rg_ref, p_ref, hid_ref, out_ref = refs[2 + shards:8 + shards]
    w_scr, mix_scr, p_scr, w_sem = refs[8 + shards:]
    heads, half = a_ref.shape[0], a_ref.shape[1]
    cols = w_scr.shape[2]
    loads = [pltpu.make_async_copy(w_refs[i], w_scr.at[i], w_sem.at[i]) for i in range(shards)]
    for c in loads:
        c.start()
    rows = p_ref.shape[1]
    slot = lax.broadcasted_iota(jnp.int32, (SLOTS, rows), 0).astype(F32)
    for e in range(p_ref.shape[0]):
        p_scr[e * SLOTS:(e + 1) * SLOTS, :] = jnp.where(
            p_ref[e:e + 1, :] == slot, 1.0, 0.0).astype(BF16)
    att = jnp.concatenate([
        jnp.concatenate([
            jnp.concatenate([a_ref[2 * j][:, side], a_ref[2 * j + 1][:, side]], axis=1)
            for j in range(heads // 2)
        ], axis=1)
        for side in (slice(0, 64), slice(64, 128))
    ], axis=0)
    chips = shards // 2
    chip, core = lax.div(here_ref[0], 2), lax.rem(here_ref[0], 2)
    for c in loads:
        c.wait()
    for i in range(shards):
        turn, swapped = i % chips, i // chips
        shard = lax.rem(chip + chips - turn, chips) * 2 + (1 - core if swapped else core)
        at = pl.multiple_of(shard * cols, cols)
        mix_scr[:, pl.ds(at, cols)] = jnp.dot(att, w_scr[i], preferred_element_type=F32)
    width = mix_scr.shape[1]
    scales = []
    for part in range(4):
        at = slice(half // 2 * part, half // 2 * (part + 1))
        mixed = mix_scr[at, :]
        scale = lax.rsqrt(jnp.mean(mixed * mixed, axis=1, keepdims=True) + 1e-6)
        hidden = (res_ref[at, :].astype(F32) + mixed * scale * mg_ref[...]).astype(BF16)
        hid_ref[at, :] = hidden
        h = hidden.astype(F32)
        scales.append(lax.rsqrt(jnp.mean(h * h, axis=1, keepdims=True) + 1e-6))
    scale = jnp.concatenate(scales, axis=0)
    for j in range(0, width, 512):
        at = slice(j, j + 512)
        routed = (hid_ref[:, at].astype(F32) * scale * rg_ref[:, at]).astype(BF16)
        out_ref[:, at] = jnp.dot(p_scr[...], routed, preferred_element_type=F32).astype(BF16)


def project(here, att, weights, residual, mix_gain, route_gain, table):
    rows, width = residual.shape
    n = len(weights)
    return pl.pallas_call(
        project_kernel,
        out_shape=(
            jax.ShapeDtypeStruct((rows, width), BF16),
            jax.ShapeDtypeStruct((table.shape[0] * SLOTS, width), BF16),
        ),
        in_specs=[pl.BlockSpec(memory_space=pltpu.SMEM), vspec()] + [hspec()] * n + [vspec()] * 4,
        out_specs=(vspec(), vspec()),
        scratch_shapes=[
            pltpu.VMEM((n,) + weights[0].shape, BF16),
            pltpu.VMEM((rows, width), F32),
            pltpu.VMEM((table.shape[0] * SLOTS, rows), BF16),
            pltpu.SemaphoreType.DMA((n,)),
        ],
        compiler_params=vmem(42),
        name="project",
    )(here, att, *weights, residual, mix_gain, route_gain, table)


def expert_kernel(x_ref, g_ref, u_ref, d_ref, o_ref, act_scr):
    ft, dt = 512, 512

    def hidden(f, _):
        at = pl.ds(pl.multiple_of(f * ft, ft), ft)
        gate = jnp.dot(x_ref[...], g_ref[:, at], preferred_element_type=F32)
        upper = jnp.dot(x_ref[...], u_ref[:, at], preferred_element_type=F32)
        act_scr[:, at] = (gate / (1.0 + jnp.exp(-gate)) * upper).astype(BF16)
        return 0

    lax.fori_loop(0, act_scr.shape[1] // ft, hidden, 0)

    def result(j, _):
        at = pl.ds(pl.multiple_of(j * dt, dt), dt)
        o_ref[:, at] = jnp.dot(act_scr[...], d_ref[:, at], preferred_element_type=F32).astype(BF16)
        return 0

    lax.fori_loop(0, o_ref.shape[1] // dt, result, 0)


def expert(x, gate, up, down):
    rows, width = x.shape
    ff = gate.shape[1]
    return pl.pallas_call(
        expert_kernel,
        out_shape=jax.ShapeDtypeStruct((rows, width), BF16),
        in_specs=[vspec()] * 4,
        out_specs=vspec(),
        scratch_shapes=[pltpu.VMEM((rows, ff), BF16)],
        compiler_params=vmem(26),
        cost_estimate=pl.CostEstimate(
            flops=6 * rows * width * ff, transcendentals=rows * ff, bytes_accessed=20000000),
        name="expert",
    )(x, gate, up, down)


def finish_kernel(c_ref, x_ref, hid_ref, og_ref, o_ref, o_scr, o_sem):
    n, _, ct = o_scr.shape
    stores = [
        pltpu.make_async_copy(o_scr.at[j], o_ref.at[:, j * ct:(j + 1) * ct], o_sem.at[j])
        for j in range(n)
    ]
    for j in range(n):
        at = slice(j * ct, (j + 1) * ct)
        combined = jnp.dot(c_ref[...], x_ref[:, at], preferred_element_type=F32)
        o_scr[j] = (hid_ref[:, at].astype(F32) + combined * og_ref[:, at]).astype(BF16)
        stores[j].start()
    for c in stores:
        c.wait()


def finish(table, x, hidden, out_gain, ct=512):
    rows, width = hidden.shape
    n = width // ct
    return pl.pallas_call(
        finish_kernel,
        out_shape=jax.ShapeDtypeStruct(hidden.shape, BF16),
        in_specs=[vspec()] * 4,
        out_specs=hspec(),
        scratch_shapes=[pltpu.VMEM((n, rows, ct), BF16), pltpu.SemaphoreType.DMA((n,))],
        compiler_params=vmem(16),
        name="finish",
    )(table, x, hidden, out_gain)


def swap(x):
    return lax.all_to_all(x, "sp", split_axis=0, concat_axis=0, tiled=True)


def gather_shards(x):
    n = lax.axis_size("dp")
    chips = n // 2
    own = [x]
    for k in range(1, chips):
        own.append(
            lax.ppermute(x, "dp", [(d, (d // 2 + k) % chips * 2 + d % 2) for d in range(n)]))
    other = [lax.ppermute(t, "dp", [(d, d ^ 1) for d in range(n)]) for t in own]
    return own + other, lax.axis_index("dp").astype(jnp.int32)[None]


def layer(
    residual,
    queries,
    key_vectors,
    value_vectors,
    gate_cache,
    out_weight,
    mix_gain,
    route_gain,
    out_gain,
    routes,
    group_share,
    expert_share,
    gate_proj,
    up_proj,
    down_proj,
):
    experts = lax.axis_size("sp")
    width = residual.shape[2]
    weights, here = gather_shards(out_weight)
    packed = pack(queries, key_vectors, value_vectors, gate_cache[0].T)
    arrived = swap(packed)
    table, back = route_tables(routes[0].T, group_share, expert_share[0].T, experts)
    attended = attend(arrived)
    att = swap(attended)
    hidden, rows_out = project(
        here, att, weights, residual[0], mix_gain[None], route_gain[None], table)

    def exchange(x):
        return swap(x.reshape(experts, SLOTS, width)).reshape(x.shape)

    result = expert(exchange(rows_out), gate_proj[0], up_proj[0], down_proj[0])
    return finish(back, exchange(result), hidden, out_gain[None])[None]


def solution(mesh):
    placed = (
        P("dp", "sp", None),
        P("dp", "sp", None),
        P("dp", "sp", None),
        P("dp", "sp", None),
        P("dp", "sp", None),
        P(None, "dp"),
        P(),
        P(),
        P(),
        P("dp", "sp", None),
        P("dp", "sp"),
        P("dp", "sp", None),
        P("sp", None, None),
        P("sp", None, None),
        P("sp", None, None),
    )
    return jax.shard_map(
        layer, mesh=mesh, in_specs=placed, out_specs=P("dp", "sp", None), check_vma=False
    )
```

```python
import jax
import jax.numpy as jnp
from jax import lax
from jax.experimental import pallas as pl
from jax.experimental.pallas import tpu as pltpu
from jax.sharding import PartitionSpec as P


F32 = jnp.float32
BF16 = jnp.bfloat16
HD = 64
SLOTS = 64
NEG = -1e30


def vmem(mib):
    return pltpu.CompilerParams(vmem_limit_bytes=mib * 1024 * 1024)


def vspec():
    return pl.BlockSpec(memory_space=pltpu.VMEM)


def hspec():
    return pl.BlockSpec(memory_space=pltpu.HBM)


def pack_kernel(q_hbm, k_hbm, v_hbm, g_hbm, o_hbm, q_ref, k_ref, v_ref, g_ref, o_ref, in_sem, g_sem,
                out_sem):
    rows = q_ref.shape[0]
    half = rows // 2
    heads = g_ref.shape[0]
    groups = out_sem.shape[0]
    step = heads // groups
    gate_load = pltpu.make_async_copy(g_hbm, g_ref, g_sem)
    gate_load.start()
    loads = []
    for part in range(2):
        for i, (src, dst) in enumerate(((q_hbm, q_ref), (k_hbm, k_ref), (v_hbm, v_ref))):
            cols = slice(512 * part, 512 * part + 512)
            loads.append(pltpu.make_async_copy(
                src.at[0, :, cols], dst.at[:, cols], in_sem.at[3 * part + i]))
            loads[-1].start()
    gate_load.wait()
    gates = g_ref[...]
    hi = gates.astype(BF16).astype(F32)
    mid = (gates - hi).astype(BF16).astype(F32)
    low = gates - hi - mid
    stores = []
    for pair in range(heads // 2):
        if pair % 4 == 0:
            for c in loads[3 * (pair // 4):3 * (pair // 4) + 3]:
                c.wait()
        cols = slice(128 * pair, 128 * pair + 128)
        q, k, v = q_ref[:, cols], k_ref[:, cols], v_ref[:, cols]
        for side in range(2):
            h = 2 * pair + side
            at = slice(64 * side, 64 * side + 64)
            o_ref[h, 0:rows, :] = jnp.concatenate([q[:, at], k[:, at]], axis=1)
            o_ref[h, rows:rows + half, :] = jnp.concatenate([v[:half, at], v[half:, at]], axis=1)
            terms = [t[h:h + 1, 128 * j:128 * j + 128] for t in (hi, mid, low) for j in range(2)]
            terms.append(jnp.zeros((10, 128), F32))
            o_ref[h, rows + half:rows + half + 16, :] = jnp.concatenate(terms, axis=0).astype(BF16)
        if (2 * pair + 2) % step == 0:
            g = (2 * pair + 2) // step - 1
            at = slice(g * step, (g + 1) * step)
            stores.append(pltpu.make_async_copy(o_ref.at[at], o_hbm.at[at], out_sem.at[g]))
            stores[-1].start()
    for c in stores:
        c.wait()


def pack(q, k, v, g):
    heads, rows = g.shape
    shape = (heads, rows + rows // 2 + 16, 128)
    return pl.pallas_call(
        pack_kernel,
        out_shape=jax.ShapeDtypeStruct(shape, BF16),
        in_specs=[hspec()] * 4,
        out_specs=hspec(),
        scratch_shapes=[pltpu.VMEM(q.shape[1:], BF16)] * 3 + [
            pltpu.VMEM(g.shape, F32),
            pltpu.VMEM(shape, BF16),
            pltpu.SemaphoreType.DMA((6,)),
            pltpu.SemaphoreType.DMA,
            pltpu.SemaphoreType.DMA((4,)),
        ],
        compiler_params=vmem(63),
        name="pack",
    )(q, k, v, g)


TILE = 512
CHUNK = 1024


def attend_kernel(x_ref, o_ref, q_scr, k_scr, v_scr, buf_a, buf_b):
    blocks = x_ref.shape[0]
    rows = (x_ref.shape[1] - 16) * 2 // 3
    half = rows // 2
    lane = lax.broadcasted_iota(jnp.int32, (rows, 64), 1)
    minus = jnp.where(lane < 3, -1.0, 0.0).astype(BF16)
    ones = jnp.where(lane < 1, 1.0, 0.0).astype(BF16)
    pr = lax.broadcasted_iota(jnp.int32, (16, 128), 0)
    pc = lax.broadcasted_iota(jnp.int32, (16, 128), 1)
    picks = [
        jnp.where((pr == 2 * (pc - 64) + j) & (pc >= 64) & (pc < 67), 1.0, 0.0).astype(BF16)
        for j in range(2)
    ]
    nt = (((1,), (1,)), ((), ()))
    tn = (((0,), (0,)), ((), ()))

    def prepare(b):
        base = b * rows
        qk = x_ref[b, 0:rows, :]
        q = (qk[:, 0:64].astype(F32) * (HD ** -0.5)).astype(BF16)
        q_scr[base:base + rows, :] = jnp.concatenate([q, minus], axis=1)
        terms = x_ref[b, rows + half:rows + half + 16, :]
        for j in range(2):
            ext = lax.dot_general(terms, picks[j], tn, preferred_element_type=F32).astype(BF16)
            at = slice(half * j, half * j + half)
            k_scr[base + half * j:base + half * j + half, :] = jnp.concatenate(
                [qk[at, 64:128], ext[:, 64:128]], axis=1)
        v = x_ref[b, rows:rows + half, :]
        v_scr[base:base + half, :] = jnp.concatenate([v[:, 0:64], ones[:half]], axis=1)
        v_scr[base + half:base + rows, :] = jnp.concatenate([v[:, 64:128], ones[:half]], axis=1)

    def score(q0, qn, k0, kn):
        return lax.dot_general(
            q_scr[q0:q0 + qn, :], k_scr[k0:k0 + kn, :], nt, preferred_element_type=F32)

    def top_of(s, m=None):
        for j in range(s.shape[1] // 128):
            t = s[:, 128 * j:128 * j + 128]
            m = t if m is None else jnp.maximum(m, t)
        return m

    def masked(s, off):
        r = lax.broadcasted_iota(jnp.int32, s.shape, 0) + off
        c = lax.broadcasted_iota(jnp.int32, s.shape, 1)
        return jnp.where(c <= r, s, NEG)

    hq = TILE // 2

    def scores_of(qi, buf):
        q0, m = qi * TILE, None
        for k0 in range(0, q0, CHUNK):
            kn = min(CHUNK, q0 - k0)
            s = score(q0, TILE, k0, kn)
            buf[:, k0:k0 + kn] = s
            m = top_of(s, m)
            yield m
        s1 = masked(score(q0, hq, q0, hq), 0)
        s2 = masked(score(q0 + hq, hq, q0, TILE), hq)
        buf[0:hq, q0:q0 + hq] = s1
        buf[hq:TILE, q0:q0 + TILE] = s2
        d = jnp.concatenate([top_of(s1), top_of(s2)], axis=0)
        yield d if m is None else jnp.maximum(m, d)

    def mix_of(qi, buf, m):
        q0 = qi * TILE
        acc = jnp.zeros((TILE, 128), F32)
        for k0 in range(0, q0, CHUNK):
            at = slice(k0, min(k0 + CHUNK, q0))
            p = jnp.exp(buf[:, at] - m).astype(BF16)
            acc = acc + jnp.dot(p, v_scr[at, :], preferred_element_type=F32)
            yield acc
        p1 = jnp.exp(buf[0:hq, q0:q0 + hq] - m[0:hq]).astype(BF16)
        p2 = jnp.exp(buf[hq:TILE, q0:q0 + TILE] - m[hq:]).astype(BF16)
        a1 = jnp.dot(p1, v_scr[q0:q0 + hq, :], preferred_element_type=F32)
        a2 = jnp.dot(p2, v_scr[q0:q0 + TILE, :], preferred_element_type=F32)
        yield acc + jnp.concatenate([a1, a2], axis=0)

    per = TILE // rows

    def store(qi, acc):
        out = acc[:, 0:64] * (1.0 / acc[:, 64:65])
        for j in range(per):
            top = out[j * rows:j * rows + half]
            bottom = out[j * rows + half:(j + 1) * rows]
            o_ref[per * qi + j] = jnp.concatenate([top, bottom], axis=1).astype(BF16)

    n = blocks // per
    bufs = [buf_a, buf_b]
    m_old = None
    for qi in range(n + 1):
        first, second = iter(()), iter(())
        if qi < n:
            for b in range(per):
                prepare(qi * per + b)
            first = scores_of(qi, bufs[qi % 2])
        if qi:
            second = mix_of(qi - 1, bufs[(qi - 1) % 2], m_old)
        m = acc = None
        while True:
            a, b = next(first, None), next(second, None)
            if a is None and b is None:
                break
            m = m if a is None else a
            acc = acc if b is None else b
        if m is not None:
            m_old = jnp.max(m, axis=1, keepdims=True)
        if acc is not None:
            store(qi - 1, acc)


def attend(x):
    blocks = x.shape[0]
    rows = (x.shape[1] - 16) * 2 // 3
    length = blocks * rows
    return pl.pallas_call(
        attend_kernel,
        out_shape=jax.ShapeDtypeStruct((blocks, rows // 2, 128), BF16),
        in_specs=[vspec()],
        out_specs=vspec(),
        scratch_shapes=[
            pltpu.VMEM((length, 128), BF16),
            pltpu.VMEM((length, 128), BF16),
            pltpu.VMEM((length, 128), BF16),
            pltpu.VMEM((TILE, length), F32),
            pltpu.VMEM((TILE, length), F32),
        ],
        compiler_params=pltpu.CompilerParams(vmem_limit_bytes=54000000),
        cost_estimate=pl.CostEstimate(
            flops=4 * length * length * 64, transcendentals=length * length // 2, bytes_accessed=4000000),
        name="attend",
    )(x)


def route_kernel(r_ref, gs_ref, es_ref, p_ref, c_ref):
    rows = r_ref.shape[1]
    experts = p_ref.shape[0]
    fill = jnp.zeros((3, rows), F32)
    columns = jnp.concatenate([r_ref[...].astype(F32), gs_ref[...], es_ref[...], fill], axis=0)
    columns = jnp.concatenate([columns, jnp.zeros((120, rows), F32)], axis=0).T
    e0, e1 = columns[:, 0:1].astype(jnp.int32), columns[:, 1:2].astype(jnp.int32)
    lane = lax.broadcasted_iota(jnp.int32, (rows, 128), 1)
    named = jnp.where((lane == e0) | (lane == e1), 1.0, 0.0)
    ri = lax.broadcasted_iota(jnp.int32, (rows, rows), 0)
    ci = lax.broadcasted_iota(jnp.int32, (rows, rows), 1)
    before = jnp.where(ci < ri, 1.0, 0.0).astype(BF16)
    rank = jnp.dot(before, named.astype(BF16), preferred_element_type=F32)
    p_ref[...] = jnp.where(named > 0, rank, -1.0).T[:experts]
    share, s0, s1 = columns[:, 2:3], columns[:, 3:4], columns[:, 4:5]
    total = s0 + s1
    w0, w1 = share * s0 / total, share * s1 / total
    k0 = jnp.sum(jnp.where(lane == e0, rank, 0.0), axis=1, keepdims=True).astype(jnp.int32)
    k1 = jnp.sum(jnp.where(lane == e1, rank, 0.0), axis=1, keepdims=True).astype(jnp.int32)
    at = lax.broadcasted_iota(jnp.int32, (rows, experts * SLOTS), 1)
    w = jnp.where(at == e0 * SLOTS + k0, w0, jnp.where(at == e1 * SLOTS + k1, w1, 0.0))
    c_ref[...] = w.astype(BF16)


def route_tables(routes, group_share, expert_share, experts):
    rows = routes.shape[1]
    n = experts * SLOTS
    return pl.pallas_call(
        route_kernel,
        out_shape=(jax.ShapeDtypeStruct((experts, rows), F32), jax.ShapeDtypeStruct((rows, n), BF16)),
        in_specs=[vspec()] * 3,
        out_specs=(vspec(),) * 2,
        compiler_params=vmem(12),
        name="route_tables",
    )(routes, group_share, expert_share)


def project_kernel(*refs):
    shards = len(refs) - 12
    here_ref, a_ref = refs[0:2]
    w_refs = refs[2:2 + shards]
    res_ref, mg_ref, rg_ref, p_ref, hid_ref, out_ref = refs[2 + shards:8 + shards]
    w_scr, mix_scr, p_scr, w_sem = refs[8 + shards:]
    heads, half = a_ref.shape[0], a_ref.shape[1]
    cols = w_scr.shape[2]
    loads = [pltpu.make_async_copy(w_refs[i], w_scr.at[i], w_sem.at[i]) for i in range(shards)]
    for c in loads:
        c.start()
    rows = p_ref.shape[1]
    slot = lax.broadcasted_iota(jnp.int32, (SLOTS, rows), 0).astype(F32)
    for e in range(p_ref.shape[0]):
        p_scr[e * SLOTS:(e + 1) * SLOTS, :] = jnp.where(
            p_ref[e:e + 1, :] == slot, 1.0, 0.0).astype(BF16)
    att = jnp.concatenate([
        jnp.concatenate([
            jnp.concatenate([a_ref[2 * j][:, side], a_ref[2 * j + 1][:, side]], axis=1)
            for j in range(heads // 2)
        ], axis=1)
        for side in (slice(0, 64), slice(64, 128))
    ], axis=0)
    chips = shards // 2
    chip, core = lax.div(here_ref[0], 2), lax.rem(here_ref[0], 2)
    for c in loads:
        c.wait()
    for i in range(shards):
        turn, swapped = i % chips, i // chips
        shard = lax.rem(chip + chips - turn, chips) * 2 + (1 - core if swapped else core)
        at = pl.multiple_of(shard * cols, cols)
        mix_scr[:, pl.ds(at, cols)] = jnp.dot(att, w_scr[i], preferred_element_type=F32)
    width = mix_scr.shape[1]
    scales = []
    for part in range(4):
        at = slice(half // 2 * part, half // 2 * (part + 1))
        mixed = mix_scr[at, :]
        scale = lax.rsqrt(jnp.mean(mixed * mixed, axis=1, keepdims=True) + 1e-6)
        hidden = (res_ref[at, :].astype(F32) + mixed * scale * mg_ref[...]).astype(BF16)
        hid_ref[at, :] = hidden
        h = hidden.astype(F32)
        scales.append(lax.rsqrt(jnp.mean(h * h, axis=1, keepdims=True) + 1e-6))
    scale = jnp.concatenate(scales, axis=0)
    for j in range(0, width, 512):
        at = slice(j, j + 512)
        routed = (hid_ref[:, at].astype(F32) * scale * rg_ref[:, at]).astype(BF16)
        out_ref[:, at] = jnp.dot(p_scr[...], routed, preferred_element_type=F32).astype(BF16)


def project(here, att, weights, residual, mix_gain, route_gain, table):
    rows, width = residual.shape
    n = len(weights)
    return pl.pallas_call(
        project_kernel,
        out_shape=(
            jax.ShapeDtypeStruct((rows, width), BF16),
            jax.ShapeDtypeStruct((table.shape[0] * SLOTS, width), BF16),
        ),
        in_specs=[pl.BlockSpec(memory_space=pltpu.SMEM), vspec()] + [hspec()] * n + [vspec()] * 4,
        out_specs=(vspec(), vspec()),
        scratch_shapes=[
            pltpu.VMEM((n,) + weights[0].shape, BF16),
            pltpu.VMEM((rows, width), F32),
            pltpu.VMEM((table.shape[0] * SLOTS, rows), BF16),
            pltpu.SemaphoreType.DMA((n,)),
        ],
        compiler_params=vmem(42),
        name="project",
    )(here, att, *weights, residual, mix_gain, route_gain, table)


def expert_kernel(x_ref, g_ref, u_ref, d_ref, o_ref, act_scr):
    ft, dt = 512, 512

    def hidden(f, _):
        at = pl.ds(pl.multiple_of(f * ft, ft), ft)
        gate = jnp.dot(x_ref[...], g_ref[:, at], preferred_element_type=F32)
        upper = jnp.dot(x_ref[...], u_ref[:, at], preferred_element_type=F32)
        act_scr[:, at] = (gate / (1.0 + jnp.exp(-gate)) * upper).astype(BF16)
        return 0

    lax.fori_loop(0, act_scr.shape[1] // ft, hidden, 0)

    def result(j, _):
        at = pl.ds(pl.multiple_of(j * dt, dt), dt)
        o_ref[:, at] = jnp.dot(act_scr[...], d_ref[:, at], preferred_element_type=F32).astype(BF16)
        return 0

    lax.fori_loop(0, o_ref.shape[1] // dt, result, 0)


def expert(x, gate, up, down):
    rows, width = x.shape
    ff = gate.shape[1]
    return pl.pallas_call(
        expert_kernel,
        out_shape=jax.ShapeDtypeStruct((rows, width), BF16),
        in_specs=[vspec()] * 4,
        out_specs=vspec(),
        scratch_shapes=[pltpu.VMEM((rows, ff), BF16)],
        compiler_params=vmem(26),
        cost_estimate=pl.CostEstimate(
            flops=6 * rows * width * ff, transcendentals=rows * ff, bytes_accessed=20000000),
        name="expert",
    )(x, gate, up, down)


def finish_kernel(c_ref, x_ref, hid_ref, og_ref, o_ref, o_scr, o_sem):
    n, _, ct = o_scr.shape
    stores = [
        pltpu.make_async_copy(o_scr.at[j], o_ref.at[:, j * ct:(j + 1) * ct], o_sem.at[j])
        for j in range(n)
    ]
    for j in range(n):
        at = slice(j * ct, (j + 1) * ct)
        combined = jnp.dot(c_ref[...], x_ref[:, at], preferred_element_type=F32)
        o_scr[j] = (hid_ref[:, at].astype(F32) + combined * og_ref[:, at]).astype(BF16)
        stores[j].start()
    for c in stores:
        c.wait()


def finish(table, x, hidden, out_gain, ct=512):
    rows, width = hidden.shape
    n = width // ct
    return pl.pallas_call(
        finish_kernel,
        out_shape=jax.ShapeDtypeStruct(hidden.shape, BF16),
        in_specs=[vspec()] * 4,
        out_specs=hspec(),
        scratch_shapes=[pltpu.VMEM((n, rows, ct), BF16), pltpu.SemaphoreType.DMA((n,))],
        compiler_params=vmem(16),
        name="finish",
    )(table, x, hidden, out_gain)


def swap(x):
    return lax.all_to_all(x, "sp", split_axis=0, concat_axis=0, tiled=True)


def gather_shards(x):
    n = lax.axis_size("dp")
    chips = n // 2
    own = [x]
    for k in range(1, chips):
        own.append(
            lax.ppermute(x, "dp", [(d, (d // 2 + k) % chips * 2 + d % 2) for d in range(n)]))
    other = [lax.ppermute(t, "dp", [(d, d ^ 1) for d in range(n)]) for t in own]
    return own + other, lax.axis_index("dp").astype(jnp.int32)[None]


def layer(
    residual,
    queries,
    key_vectors,
    value_vectors,
    gate_cache,
    out_weight,
    mix_gain,
    route_gain,
    out_gain,
    routes,
    group_share,
    expert_share,
    gate_proj,
    up_proj,
    down_proj,
):
    experts = lax.axis_size("sp")
    width = residual.shape[2]
    weights, here = gather_shards(out_weight)
    packed = pack(queries, key_vectors, value_vectors, gate_cache[0].T)
    arrived = swap(packed)
    table, back = route_tables(routes[0].T, group_share, expert_share[0].T, experts)
    attended = attend(arrived)
    att = swap(attended)
    hidden, rows_out = project(
        here, att, weights, residual[0], mix_gain[None], route_gain[None], table)

    def exchange(x):
        return swap(x.reshape(experts, SLOTS, width)).reshape(x.shape)

    result = expert(exchange(rows_out), gate_proj[0], up_proj[0], down_proj[0])
    return finish(back, exchange(result), hidden, out_gain[None])[None]


def solution(mesh):
    placed = (
        P("dp", "sp", None),
        P("dp", "sp", None),
        P("dp", "sp", None),
        P("dp", "sp", None),
        P("dp", "sp", None),
        P(None, "dp"),
        P(),
        P(),
        P(),
        P("dp", "sp", None),
        P("dp", "sp"),
        P("dp", "sp", None),
        P("sp", None, None),
        P("sp", None, None),
        P("sp", None, None),
    )
    return jax.shard_map(
        layer, mesh=mesh, in_specs=placed, out_specs=P("dp", "sp", None), check_vma=False
    )
```

```python
import jax
import jax.numpy as jnp
from jax import lax
from jax.experimental import pallas as pl
from jax.experimental.pallas import tpu as pltpu
from jax.sharding import PartitionSpec as P


F32 = jnp.float32
BF16 = jnp.bfloat16
HD = 64
SLOTS = 64
NEG = -1e30


def vmem(mib):
    return pltpu.CompilerParams(vmem_limit_bytes=mib * 1024 * 1024)


def vspec():
    return pl.BlockSpec(memory_space=pltpu.VMEM)


def hspec():
    return pl.BlockSpec(memory_space=pltpu.HBM)


def pack_kernel(q_hbm, k_hbm, v_hbm, g_hbm, o_hbm, q_ref, k_ref, v_ref, g_ref, o_ref, in_sem, g_sem,
                out_sem):
    rows = q_ref.shape[0]
    half = rows // 2
    heads = g_ref.shape[0]
    groups = out_sem.shape[0]
    step = heads // groups
    gate_load = pltpu.make_async_copy(g_hbm, g_ref, g_sem)
    gate_load.start()
    loads = []
    for part in range(2):
        for i, (src, dst) in enumerate(((q_hbm, q_ref), (k_hbm, k_ref), (v_hbm, v_ref))):
            cols = slice(512 * part, 512 * part + 512)
            loads.append(pltpu.make_async_copy(
                src.at[0, :, cols], dst.at[:, cols], in_sem.at[3 * part + i]))
            loads[-1].start()
    gate_load.wait()
    gates = g_ref[...]
    hi = gates.astype(BF16).astype(F32)
    mid = (gates - hi).astype(BF16).astype(F32)
    low = gates - hi - mid
    stores = []
    for pair in range(heads // 2):
        if pair % 4 == 0:
            for c in loads[3 * (pair // 4):3 * (pair // 4) + 3]:
                c.wait()
        cols = slice(128 * pair, 128 * pair + 128)
        q, k, v = q_ref[:, cols], k_ref[:, cols], v_ref[:, cols]
        for side in range(2):
            h = 2 * pair + side
            at = slice(64 * side, 64 * side + 64)
            o_ref[h, 0:rows, :] = jnp.concatenate([q[:, at], k[:, at]], axis=1)
            o_ref[h, rows:rows + half, :] = jnp.concatenate([v[:half, at], v[half:, at]], axis=1)
            terms = [t[h:h + 1, 128 * j:128 * j + 128] for t in (hi, mid, low) for j in range(2)]
            terms.append(jnp.zeros((10, 128), F32))
            o_ref[h, rows + half:rows + half + 16, :] = jnp.concatenate(terms, axis=0).astype(BF16)
        if (2 * pair + 2) % step == 0:
            g = (2 * pair + 2) // step - 1
            at = slice(g * step, (g + 1) * step)
            stores.append(pltpu.make_async_copy(o_ref.at[at], o_hbm.at[at], out_sem.at[g]))
            stores[-1].start()
    for c in stores:
        c.wait()


def pack(q, k, v, g):
    heads, rows = g.shape
    shape = (heads, rows + rows // 2 + 16, 128)
    return pl.pallas_call(
        pack_kernel,
        out_shape=jax.ShapeDtypeStruct(shape, BF16),
        in_specs=[hspec()] * 4,
        out_specs=hspec(),
        scratch_shapes=[pltpu.VMEM(q.shape[1:], BF16)] * 3 + [
            pltpu.VMEM(g.shape, F32),
            pltpu.VMEM(shape, BF16),
            pltpu.SemaphoreType.DMA((6,)),
            pltpu.SemaphoreType.DMA,
            pltpu.SemaphoreType.DMA((4,)),
        ],
        compiler_params=vmem(63),
        name="pack",
    )(q, k, v, g)


TILE = 512


def attend_kernel(x_ref, o_ref, q_scr, k_scr, v_scr, buf_a, buf_b):
    blocks = x_ref.shape[0]
    rows = (x_ref.shape[1] - 16) * 2 // 3
    half = rows // 2
    lane = lax.broadcasted_iota(jnp.int32, (rows, 64), 1)
    minus = jnp.where(lane < 3, -1.0, 0.0).astype(BF16)
    ones = jnp.where(lane < 1, 1.0, 0.0).astype(BF16)
    pr = lax.broadcasted_iota(jnp.int32, (16, 128), 0)
    pc = lax.broadcasted_iota(jnp.int32, (16, 128), 1)
    picks = [
        jnp.where((pr == 2 * (pc - 64) + j) & (pc >= 64) & (pc < 67), 1.0, 0.0).astype(BF16)
        for j in range(2)
    ]
    nt = (((1,), (1,)), ((), ()))
    tn = (((0,), (0,)), ((), ()))

    def prepare(b):
        base = b * rows
        qk = x_ref[b, 0:rows, :]
        q = (qk[:, 0:64].astype(F32) * (HD ** -0.5)).astype(BF16)
        q_scr[base:base + rows, :] = jnp.concatenate([q, minus], axis=1)
        terms = x_ref[b, rows + half:rows + half + 16, :]
        for j in range(2):
            ext = lax.dot_general(terms, picks[j], tn, preferred_element_type=F32).astype(BF16)
            at = slice(half * j, half * j + half)
            k_scr[base + half * j:base + half * j + half, :] = jnp.concatenate(
                [qk[at, 64:128], ext[:, 64:128]], axis=1)
        v = x_ref[b, rows:rows + half, :]
        v_scr[base:base + half, :] = jnp.concatenate([v[:, 0:64], ones[:half]], axis=1)
        v_scr[base + half:base + rows, :] = jnp.concatenate([v[:, 64:128], ones[:half]], axis=1)

    def score(q0, qn, k0, kn):
        return lax.dot_general(
            q_scr[q0:q0 + qn, :], k_scr[k0:k0 + kn, :], nt, preferred_element_type=F32)

    def top_of(s, m=None):
        for j in range(s.shape[1] // 128):
            t = s[:, 128 * j:128 * j + 128]
            m = t if m is None else jnp.maximum(m, t)
        return m

    def masked(s, off):
        r = lax.broadcasted_iota(jnp.int32, s.shape, 0) + off
        c = lax.broadcasted_iota(jnp.int32, s.shape, 1)
        return jnp.where(c <= r, s, NEG)

    hq = TILE // 2

    def scores_of(qi, buf):
        q0, m = qi * TILE, None
        for k0 in range(0, q0, TILE):
            s = score(q0, TILE, k0, TILE)
            buf[:, k0:k0 + TILE] = s
            m = top_of(s, m)
            yield m
        s1 = masked(score(q0, hq, q0, hq), 0)
        s2 = masked(score(q0 + hq, hq, q0, TILE), hq)
        buf[0:hq, q0:q0 + hq] = s1
        buf[hq:TILE, q0:q0 + TILE] = s2
        d = jnp.concatenate([top_of(s1), top_of(s2)], axis=0)
        yield d if m is None else jnp.maximum(m, d)

    def mix_of(qi, buf, m):
        q0 = qi * TILE
        acc = jnp.zeros((TILE, 128), F32)
        for k0 in range(0, q0, TILE):
            p = jnp.exp(buf[:, k0:k0 + TILE] - m).astype(BF16)
            acc = acc + jnp.dot(p, v_scr[k0:k0 + TILE, :], preferred_element_type=F32)
            yield acc
        p1 = jnp.exp(buf[0:hq, q0:q0 + hq] - m[0:hq]).astype(BF16)
        p2 = jnp.exp(buf[hq:TILE, q0:q0 + TILE] - m[hq:]).astype(BF16)
        a1 = jnp.dot(p1, v_scr[q0:q0 + hq, :], preferred_element_type=F32)
        a2 = jnp.dot(p2, v_scr[q0:q0 + TILE, :], preferred_element_type=F32)
        yield acc + jnp.concatenate([a1, a2], axis=0)

    per = TILE // rows

    def store(qi, acc):
        out = acc[:, 0:64] * (1.0 / acc[:, 64:65])
        for j in range(per):
            top = out[j * rows:j * rows + half]
            bottom = out[j * rows + half:(j + 1) * rows]
            o_ref[per * qi + j] = jnp.concatenate([top, bottom], axis=1).astype(BF16)

    n = blocks // per
    bufs = [buf_a, buf_b]
    m_old = None
    for qi in range(n + 1):
        first, second = iter(()), iter(())
        if qi < n:
            for b in range(per):
                prepare(qi * per + b)
            first = scores_of(qi, bufs[qi % 2])
        if qi:
            second = mix_of(qi - 1, bufs[(qi - 1) % 2], m_old)
        m = acc = None
        while True:
            a, b = next(first, None), next(second, None)
            if a is None and b is None:
                break
            m = m if a is None else a
            acc = acc if b is None else b
        if m is not None:
            m_old = jnp.max(m, axis=1, keepdims=True)
        if acc is not None:
            store(qi - 1, acc)


def attend(x):
    blocks = x.shape[0]
    rows = (x.shape[1] - 16) * 2 // 3
    length = blocks * rows
    return pl.pallas_call(
        attend_kernel,
        out_shape=jax.ShapeDtypeStruct((blocks, rows // 2, 128), BF16),
        in_specs=[vspec()],
        out_specs=vspec(),
        scratch_shapes=[
            pltpu.VMEM((length, 128), BF16),
            pltpu.VMEM((length, 128), BF16),
            pltpu.VMEM((length, 128), BF16),
            pltpu.VMEM((TILE, length), F32),
            pltpu.VMEM((TILE, length), F32),
        ],
        compiler_params=pltpu.CompilerParams(vmem_limit_bytes=54000000),
        cost_estimate=pl.CostEstimate(
            flops=4 * length * length * 64, transcendentals=length * length // 2, bytes_accessed=4000000),
        name="attend",
    )(x)


def route_kernel(r_ref, gs_ref, es_ref, p_ref, c_ref):
    rows = r_ref.shape[1]
    experts = p_ref.shape[0]
    fill = jnp.zeros((3, rows), F32)
    columns = jnp.concatenate([r_ref[...].astype(F32), gs_ref[...], es_ref[...], fill], axis=0)
    columns = jnp.concatenate([columns, jnp.zeros((120, rows), F32)], axis=0).T
    e0, e1 = columns[:, 0:1].astype(jnp.int32), columns[:, 1:2].astype(jnp.int32)
    lane = lax.broadcasted_iota(jnp.int32, (rows, 128), 1)
    named = jnp.where((lane == e0) | (lane == e1), 1.0, 0.0)
    ri = lax.broadcasted_iota(jnp.int32, (rows, rows), 0)
    ci = lax.broadcasted_iota(jnp.int32, (rows, rows), 1)
    before = jnp.where(ci < ri, 1.0, 0.0).astype(BF16)
    rank = jnp.dot(before, named.astype(BF16), preferred_element_type=F32)
    p_ref[...] = jnp.where(named > 0, rank, -1.0).T[:experts]
    share, s0, s1 = columns[:, 2:3], columns[:, 3:4], columns[:, 4:5]
    total = s0 + s1
    w0, w1 = share * s0 / total, share * s1 / total
    k0 = jnp.sum(jnp.where(lane == e0, rank, 0.0), axis=1, keepdims=True).astype(jnp.int32)
    k1 = jnp.sum(jnp.where(lane == e1, rank, 0.0), axis=1, keepdims=True).astype(jnp.int32)
    at = lax.broadcasted_iota(jnp.int32, (rows, experts * SLOTS), 1)
    w = jnp.where(at == e0 * SLOTS + k0, w0, jnp.where(at == e1 * SLOTS + k1, w1, 0.0))
    c_ref[...] = w.astype(BF16)


def route_tables(routes, group_share, expert_share, experts):
    rows = routes.shape[1]
    n = experts * SLOTS
    return pl.pallas_call(
        route_kernel,
        out_shape=(jax.ShapeDtypeStruct((experts, rows), F32), jax.ShapeDtypeStruct((rows, n), BF16)),
        in_specs=[vspec()] * 3,
        out_specs=(vspec(),) * 2,
        compiler_params=vmem(12),
        name="route_tables",
    )(routes, group_share, expert_share)


def project_kernel(*refs):
    shards = len(refs) - 12
    here_ref, a_ref = refs[0:2]
    w_refs = refs[2:2 + shards]
    res_ref, mg_ref, rg_ref, p_ref, hid_ref, out_ref = refs[2 + shards:8 + shards]
    w_scr, mix_scr, p_scr, w_sem = refs[8 + shards:]
    heads, half = a_ref.shape[0], a_ref.shape[1]
    cols = w_scr.shape[2]
    loads = [pltpu.make_async_copy(w_refs[i], w_scr.at[i], w_sem.at[i]) for i in range(shards)]
    for c in loads:
        c.start()
    rows = p_ref.shape[1]
    slot = lax.broadcasted_iota(jnp.int32, (SLOTS, rows), 0).astype(F32)
    for e in range(p_ref.shape[0]):
        p_scr[e * SLOTS:(e + 1) * SLOTS, :] = jnp.where(
            p_ref[e:e + 1, :] == slot, 1.0, 0.0).astype(BF16)
    att = jnp.concatenate([
        jnp.concatenate([
            jnp.concatenate([a_ref[2 * j][:, side], a_ref[2 * j + 1][:, side]], axis=1)
            for j in range(heads // 2)
        ], axis=1)
        for side in (slice(0, 64), slice(64, 128))
    ], axis=0)
    chips = shards // 2
    chip, core = lax.div(here_ref[0], 2), lax.rem(here_ref[0], 2)
    for c in loads:
        c.wait()
    for i in range(shards):
        turn, swapped = i % chips, i // chips
        shard = lax.rem(chip + chips - turn, chips) * 2 + (1 - core if swapped else core)
        at = pl.multiple_of(shard * cols, cols)
        mix_scr[:, pl.ds(at, cols)] = jnp.dot(att, w_scr[i], preferred_element_type=F32)
    width = mix_scr.shape[1]
    scales = []
    for part in range(4):
        at = slice(half // 2 * part, half // 2 * (part + 1))
        mixed = mix_scr[at, :]
        scale = lax.rsqrt(jnp.mean(mixed * mixed, axis=1, keepdims=True) + 1e-6)
        hidden = (res_ref[at, :].astype(F32) + mixed * scale * mg_ref[...]).astype(BF16)
        hid_ref[at, :] = hidden
        h = hidden.astype(F32)
        scales.append(lax.rsqrt(jnp.mean(h * h, axis=1, keepdims=True) + 1e-6))
    scale = jnp.concatenate(scales, axis=0)
    for j in range(0, width, 512):
        at = slice(j, j + 512)
        routed = (hid_ref[:, at].astype(F32) * scale * rg_ref[:, at]).astype(BF16)
        out_ref[:, at] = jnp.dot(p_scr[...], routed, preferred_element_type=F32).astype(BF16)


def project(here, att, weights, residual, mix_gain, route_gain, table):
    rows, width = residual.shape
    n = len(weights)
    return pl.pallas_call(
        project_kernel,
        out_shape=(
            jax.ShapeDtypeStruct((rows, width), BF16),
            jax.ShapeDtypeStruct((table.shape[0] * SLOTS, width), BF16),
        ),
        in_specs=[pl.BlockSpec(memory_space=pltpu.SMEM), vspec()] + [hspec()] * n + [vspec()] * 4,
        out_specs=(vspec(), vspec()),
        scratch_shapes=[
            pltpu.VMEM((n,) + weights[0].shape, BF16),
            pltpu.VMEM((rows, width), F32),
            pltpu.VMEM((table.shape[0] * SLOTS, rows), BF16),
            pltpu.SemaphoreType.DMA((n,)),
        ],
        compiler_params=vmem(42),
        name="project",
    )(here, att, *weights, residual, mix_gain, route_gain, table)


def expert_kernel(x_ref, g_ref, u_ref, d_ref, o_ref, act_scr):
    ft, dt = 512, 512

    def hidden(f, _):
        at = pl.ds(pl.multiple_of(f * ft, ft), ft)
        gate = jnp.dot(x_ref[...], g_ref[:, at], preferred_element_type=F32)
        upper = jnp.dot(x_ref[...], u_ref[:, at], preferred_element_type=F32)
        act_scr[:, at] = (gate / (1.0 + jnp.exp(-gate)) * upper).astype(BF16)
        return 0

    lax.fori_loop(0, act_scr.shape[1] // ft, hidden, 0)

    def result(j, _):
        at = pl.ds(pl.multiple_of(j * dt, dt), dt)
        o_ref[:, at] = jnp.dot(act_scr[...], d_ref[:, at], preferred_element_type=F32).astype(BF16)
        return 0

    lax.fori_loop(0, o_ref.shape[1] // dt, result, 0)


def expert(x, gate, up, down):
    rows, width = x.shape
    ff = gate.shape[1]
    return pl.pallas_call(
        expert_kernel,
        out_shape=jax.ShapeDtypeStruct((rows, width), BF16),
        in_specs=[vspec()] * 4,
        out_specs=vspec(),
        scratch_shapes=[pltpu.VMEM((rows, ff), BF16)],
        compiler_params=vmem(26),
        cost_estimate=pl.CostEstimate(
            flops=6 * rows * width * ff, transcendentals=rows * ff, bytes_accessed=20000000),
        name="expert",
    )(x, gate, up, down)


def finish_kernel(c_ref, x_ref, hid_ref, og_ref, o_ref, o_scr, o_sem):
    n, _, ct = o_scr.shape
    stores = [
        pltpu.make_async_copy(o_scr.at[j], o_ref.at[:, j * ct:(j + 1) * ct], o_sem.at[j])
        for j in range(n)
    ]
    for j in range(n):
        at = slice(j * ct, (j + 1) * ct)
        combined = jnp.dot(c_ref[...], x_ref[:, at], preferred_element_type=F32)
        o_scr[j] = (hid_ref[:, at].astype(F32) + combined * og_ref[:, at]).astype(BF16)
        stores[j].start()
    for c in stores:
        c.wait()


def finish(table, x, hidden, out_gain, ct=256):
    rows, width = hidden.shape
    n = width // ct
    return pl.pallas_call(
        finish_kernel,
        out_shape=jax.ShapeDtypeStruct(hidden.shape, BF16),
        in_specs=[vspec()] * 4,
        out_specs=hspec(),
        scratch_shapes=[pltpu.VMEM((n, rows, ct), BF16), pltpu.SemaphoreType.DMA((n,))],
        compiler_params=vmem(16),
        name="finish",
    )(table, x, hidden, out_gain)


def swap(x):
    return lax.all_to_all(x, "sp", split_axis=0, concat_axis=0, tiled=True)


def gather_shards(x):
    n = lax.axis_size("dp")
    chips = n // 2
    own = [x]
    for k in range(1, chips):
        own.append(
            lax.ppermute(x, "dp", [(d, (d // 2 + k) % chips * 2 + d % 2) for d in range(n)]))
    other = [lax.ppermute(t, "dp", [(d, d ^ 1) for d in range(n)]) for t in own]
    return own + other, lax.axis_index("dp").astype(jnp.int32)[None]


def layer(
    residual,
    queries,
    key_vectors,
    value_vectors,
    gate_cache,
    out_weight,
    mix_gain,
    route_gain,
    out_gain,
    routes,
    group_share,
    expert_share,
    gate_proj,
    up_proj,
    down_proj,
):
    experts = lax.axis_size("sp")
    width = residual.shape[2]
    weights, here = gather_shards(out_weight)
    packed = pack(queries, key_vectors, value_vectors, gate_cache[0].T)
    arrived = swap(packed)
    table, back = route_tables(routes[0].T, group_share, expert_share[0].T, experts)
    attended = attend(arrived)
    att = swap(attended)
    hidden, rows_out = project(
        here, att, weights, residual[0], mix_gain[None], route_gain[None], table)

    def exchange(x):
        return swap(x.reshape(experts, SLOTS, width)).reshape(x.shape)

    result = expert(exchange(rows_out), gate_proj[0], up_proj[0], down_proj[0])
    return finish(back, exchange(result), hidden, out_gain[None])[None]


def solution(mesh):
    placed = (
        P("dp", "sp", None),
        P("dp", "sp", None),
        P("dp", "sp", None),
        P("dp", "sp", None),
        P("dp", "sp", None),
        P(None, "dp"),
        P(),
        P(),
        P(),
        P("dp", "sp", None),
        P("dp", "sp"),
        P("dp", "sp", None),
        P("sp", None, None),
        P("sp", None, None),
        P("sp", None, None),
    )
    return jax.shard_map(
        layer, mesh=mesh, in_specs=placed, out_specs=P("dp", "sp", None), check_vma=False
    )
```
